256 devices in a mesh: dp: 4 (over x), kv: 32 (over z, y), tp: 2 (over core).
Axes of the slice: x: 4, y: 4, z: 8, core: 2. Of those that a mesh axis runs over, the one named last changes fastest.
Arguments:
- tokens: bfloat16 [128, 4096], P('dp', ('kv', 'tp')), may hold values from -24 to 24
- rec_state: float32 [128, 16, 128, 128], P(('dp', 'kv'), 'tp'), may hold values from -2 to 2
- norm_gain: float32 [4096], replicated, may hold values from 0.1 to 1.9
- w_query: bfloat16 [4096, 2048], P('kv', 'tp'), may hold values from -0.09375 to 0.09375
- w_forget: bfloat16 [4096, 2048], P('kv', 'tp'), may hold values from -0.09375 to 0.09375
- w_input: bfloat16 [4096, 2048], P('kv', 'tp'), may hold values from -0.09375 to 0.09375
- w_outgate: bfloat16 [4096, 2048], P('kv', 'tp'), may hold values from -0.09375 to 0.09375
- lower_bound: float32 [2048], P('tp'), may hold values from 0 to 0.9
- head_gain: float32 [2048], P('tp'), may hold values from 0.1 to 1.9
- w_heads_out: bfloat16 [2048, 4096], P(None, ('kv', 'tp')), may hold values from -0.125 to 0.125
- mixer_gain: float32 [4096], replicated, may hold values from 0.1 to 1.9
- w_gate: bfloat16 [4096, 11264], P(None, ('kv', 'tp')), may hold values from -0.09375 to 0.09375
- w_up: bfloat16 [4096, 11264], P(None, ('kv', 'tp')), may hold values from -0.09375 to 0.09375
- w_down: bfloat16 [11264, 4096], P(('kv', 'tp')), may hold values from -0.15625 to 0.15625
Outputs:
- result: bfloat16 [128, 4096], P('dp', ('kv', 'tp'))
- new_state: float32 [128, 16, 128, 128], P(('dp', 'kv'), 'tp')
The draws below stay inside these ranges and needn't reach their ends.
All inputs are finite; a program needn't handle non-finite values.
Results may differ from the reference program's by a relative error of at most 0.012.
Values may be sent and summed in bfloat16 or wider, within the bound.
No kernel may reach another device: no remote copies, remote signals or barrier semaphores. Data moves between devices by JAX's collectives and lax.ppermute only.
A program may use at most 64 MiB of HBM per device.

```python
import math
import jax
import jax.numpy as jnp
from jax import lax

D = 4096
HEAD_DIM = 128
HEADS = 16
FF = 11264
HG = 2048
BATCH = 128


def draw_tokens(key, part):
    key_rows = jax.random.fold_in(key, 11)
    key_vals = jax.random.fold_in(key, 12)
    col_scale = jnp.exp(jnp.linspace(math.log(0.5), math.log(2.0), D))[None, :]
    row_scale = jnp.exp(jax.random.uniform(key_rows, (BATCH, 1), jnp.float32, math.log(0.3), math.log(3.0)))
    values = jnp.clip(jax.random.normal(key_vals, (BATCH, D), jnp.float32), -4.0, 4.0)
    return (values * row_scale * col_scale).astype(jnp.bfloat16)


def strengthened(array, own_key, source, target, parts, factor):
    owner, partner = [(jnp.arange(array.shape[dim]) // (array.shape[dim] // parts)).reshape([-1 if axis == dim else 1 for axis in range(array.ndim)]) for dim in (source, target)]
    chosen = jax.random.permutation(own_key, parts)[partner]
    strong = (owner == chosen) | (owner == (partner + parts // 2) % parts)
    return jnp.where(strong, factor * array, array)


def block_levels(rng, shape, shards, least, top_value):
    loudness = 1.0
    for axis_at, parts in shards:
        steps = jax.random.uniform(jax.random.fold_in(jax.random.fold_in(rng, 6), axis_at), (parts,), jnp.float32, least / len(shards), top_value / len(shards))
        loudness = loudness * jnp.repeat(jnp.exp(steps), shape[axis_at] // parts).reshape((-1,) + (1,) * (len(shape) - 1 - axis_at))
    return loudness


def gaussian(key, extent, deviation, limit, shards=(), kind=jnp.bfloat16):
    drawn = deviation * jax.random.normal(key, extent, jnp.float32)
    if shards:
        drawn = drawn * block_levels(key, extent, shards, -0.22, 0.18)
    return jnp.clip(drawn, -limit, limit).astype(kind)


def noise_with(stream_key, shape, scale, bound, split, heavy, held_as=jnp.bfloat16):
    array = scale * jax.random.normal(stream_key, shape, jnp.float32)
    if split:
        array = array * block_levels(stream_key, shape, split, -0.22, 0.18)
    return jnp.clip(strengthened(array, jax.random.fold_in(stream_key, 3), *heavy), -bound, bound).astype(held_as)


def setup_inputs(seed: int = 0) -> dict:
    streams_of = jax.random.split(jax.random.key(seed), 15)
    return {
        "tokens": draw_tokens(jax.random.fold_in(streams_of[14], 71), 0),
        "rec_state": gaussian(streams_of[1], (BATCH, HEADS, HEAD_DIM, HEAD_DIM), 0.3, 2.0, ((0, 128), (1, 2)), jnp.float32),
        "norm_gain": jnp.clip(1.0 + 0.18 * jax.random.normal(streams_of[2], (D,), jnp.float32), 0.1, 1.9),
        "w_query": gaussian(streams_of[3], (D, HG), D ** -0.5, 0.09375, ((0, 32), (1, 2))),
        "w_forget": gaussian(streams_of[4], (D, HG), D ** -0.5, 0.09375, ((0, 32), (1, 2))),
        "w_input": gaussian(streams_of[5], (D, HG), D ** -0.5, 0.09375, ((0, 32), (1, 2))),
        "w_outgate": gaussian(streams_of[6], (D, HG), D ** -0.5, 0.09375, ((0, 32), (1, 2))),
        "lower_bound": jnp.clip(0.9 * jax.random.uniform(streams_of[7], (HG,), jnp.float32) ** block_levels(streams_of[7], (HG,), ((0, 2),), -0.2, 0.2), 0.0, 0.9),
        "head_gain": jnp.clip(1.0 + 0.18 * jax.random.normal(streams_of[8], (HG,), jnp.float32), 0.1, 1.9),
        "w_heads_out": gaussian(streams_of[9], (HG, D), HG ** -0.5, 0.125, ((1, 64),)),
        "mixer_gain": jnp.clip(1.0 + 0.18 * jax.random.normal(streams_of[10], (D,), jnp.float32), 0.1, 1.9),
        "w_gate": gaussian(streams_of[11], (D, FF), D ** -0.5, 0.09375, ((1, 64),)),
        "w_up": gaussian(streams_of[12], (D, FF), D ** -0.5, 0.09375, ((1, 64),)),
        "w_down": noise_with(streams_of[13], (FF, D), FF ** -0.5, 0.15625, ((0, 64),), (0, 1, 64, 4.0)),
    }


epsilon = 1e-06

def reference(tokens, rec_state, norm_gain, w_query, w_forget, w_input, w_outgate, lower_bound, head_gain, w_heads_out, mixer_gain, w_gate, w_up, w_down):
    tok_float = tokens.astype(jnp.float32)
    row_scale = lax.rsqrt(lax.optimization_barrier(jnp.mean(tok_float * tok_float, axis=1, keepdims=True)) + epsilon)
    scaled = (tok_float * norm_gain).astype(jnp.bfloat16)
    query_pre = row_scale * jnp.dot(scaled, w_query, preferred_element_type=jnp.float32)
    forget_pre = row_scale * jnp.dot(scaled, w_forget, preferred_element_type=jnp.float32)
    value_in = row_scale * jnp.dot(scaled, w_input, preferred_element_type=jnp.float32)
    gate_pre = row_scale * jnp.dot(scaled, w_outgate, preferred_element_type=jnp.float32)
    forget = lower_bound + (1.0 - lower_bound) * jax.nn.sigmoid(forget_pre)
    key_in = 1.0 - forget
    query_act = jax.nn.silu(query_pre)
    batch_rows = tokens.shape[0]
    shaped = (batch_rows, HEADS, HEAD_DIM)
    forget = forget.reshape(shaped)
    key_in = key_in.reshape(shaped)
    value_in = value_in.reshape(shaped)
    query_act = query_act.reshape(shaped)
    new_state = forget[:, :, :, None] * rec_state + key_in[:, :, :, None] * value_in[:, :, None, :]
    head_out = lax.optimization_barrier(jnp.sum(query_act[:, :, :, None] * new_state, axis=2))
    head_out = head_out * lax.rsqrt(lax.optimization_barrier(jnp.mean(head_out * head_out, axis=2, keepdims=True)) + epsilon)
    head_out = head_out * head_gain.reshape(HEADS, HEAD_DIM)
    gated = (head_out.reshape(batch_rows, HG) * jax.nn.silu(gate_pre)).astype(jnp.bfloat16)
    mixed = (tok_float + jnp.dot(gated, w_heads_out, preferred_element_type=jnp.float32)).astype(jnp.bfloat16)
    mixed_float = mixed.astype(jnp.float32)
    mixer_scale = lax.rsqrt(lax.optimization_barrier(jnp.mean(mixed_float * mixed_float, axis=1, keepdims=True)) + epsilon)
    normed = (mixed_float * mixer_scale * mixer_gain).astype(jnp.bfloat16)
    gate_val = jnp.dot(normed, w_gate, preferred_element_type=jnp.float32)
    up_val = jnp.dot(normed, w_up, preferred_element_type=jnp.float32)
    hidden = (jax.nn.silu(gate_val) * up_val).astype(jnp.bfloat16)
    result = (mixed_float + jnp.dot(hidden, w_down, preferred_element_type=jnp.float32)).astype(jnp.bfloat16)
    return (result, new_state)
```

```python
import jax
import jax.numpy as jnp
from jax import lax
from jax.sharding import Mesh
from jax.sharding import PartitionSpec as P

HEAD_DIM = 128
KV = ("kv_0", "kv_1")
KV_TP = ("kv_0", "kv_1", "tp")
DP_KV = ("dp", "kv_0", "kv_1")
SWAP = [(0, 1), (1, 0)]

epsilon = 1e-06


def exchanged(pieces, axis):
    return lax.all_to_all(pieces, axis, split_axis=0, concat_axis=0, tiled=True)


def to_everyone(value, axis):
    return exchanged(jnp.broadcast_to(value, (lax.axis_size(axis), *value.shape)), axis)


def by_core(own, other, core):
    first = jnp.where(core == 0, own, other)
    second = jnp.where(core == 0, other, own)
    return first, second


def local(
    tokens,
    rec_state,
    norm_gain,
    w_query,
    w_forget,
    w_input,
    w_outgate,
    lower_bound,
    head_gain,
    w_heads_out,
    mixer_gain,
    w_gate,
    w_up,
    w_down,
):
    bf16, f32 = jnp.bfloat16, jnp.float32
    kv_count = lax.axis_size(KV)
    core = lax.axis_index("tp")
    kv_index = lax.axis_index(KV)
    rows, cols = tokens.shape
    model_width = norm_gain.shape[0]
    heads = rec_state.shape[1]
    width = heads * HEAD_DIM
    half = rows // 2

    first, second = by_core(tokens, lax.ppermute(tokens, "tp", SWAP), core)
    block = jnp.concatenate([first, second], axis=1).astype(f32)
    gain = lax.dynamic_slice_in_dim(norm_gain, kv_index * 2 * cols, 2 * cols, 0)
    squares = jnp.sum(block * block, axis=1)
    high = squares.astype(bf16)
    low = (squares - high.astype(f32)).astype(bf16)
    scaled = (block * gain).astype(bf16)
    parts = [
        jnp.dot(scaled, w, preferred_element_type=f32).astype(bf16).reshape(rows, heads, HEAD_DIM)
        for w in (w_query, w_forget, w_input, w_outgate)
    ]
    extra = jnp.concatenate([high[:, None], low[:, None], jnp.zeros((rows, HEAD_DIM - 2), bf16)], axis=1)
    extra = jnp.broadcast_to(extra[:, None, :], (rows, heads, HEAD_DIM))
    pieces = jnp.concatenate(parts + [extra], axis=1)
    summed = jnp.sum(exchanged(pieces, KV).astype(f32), axis=0)
    row_scale = lax.rsqrt((summed[4 * heads, 0] + summed[4 * heads, 1]) / model_width + epsilon)
    scaled_sum = row_scale * summed[: 4 * heads].reshape(4, heads, HEAD_DIM)
    query_pre, forget_pre, value_in, gate_pre = [scaled_sum[i] for i in range(4)]

    bound = lower_bound.reshape(heads, HEAD_DIM)
    forget = bound + (1.0 - bound) * jax.nn.sigmoid(forget_pre)
    key_in = 1.0 - forget
    query_act = jax.nn.silu(query_pre)
    new_state = forget[:, :, None] * rec_state[0] + key_in[:, :, None] * value_in[:, None, :]
    head_out = jnp.sum(query_act[:, :, None] * new_state, axis=1)
    head_out = head_out * lax.rsqrt(jnp.mean(head_out * head_out, axis=1, keepdims=True) + epsilon)
    head_out = head_out * head_gain.reshape(heads, HEAD_DIM)
    gated = (head_out * jax.nn.silu(gate_pre)).astype(bf16)

    every_head = to_everyone(gated, KV_TP).reshape(rows, 2 * width)
    mixed = (tokens.astype(f32) + jnp.dot(every_head, w_heads_out, preferred_element_type=f32)).astype(bf16)

    packed = jnp.concatenate([mixed[:half], mixed[half:]], axis=1)
    own = to_everyone(packed, KV)
    first, second = by_core(own, lax.ppermute(own, "tp", SWAP), core)
    top = jnp.concatenate([first[:, :, :cols], second[:, :, :cols]], axis=2)
    bottom = jnp.concatenate([first[:, :, cols:], second[:, :, cols:]], axis=2)
    whole = jnp.concatenate([top, bottom], axis=1).transpose(1, 0, 2).reshape(rows, model_width)

    rows_float = whole.astype(f32)
    mixer_scale = lax.rsqrt(jnp.mean(rows_float * rows_float, axis=1, keepdims=True) + epsilon)
    normed = (rows_float * mixer_scale * mixer_gain).astype(bf16)
    gate_val = jnp.dot(normed, w_gate, preferred_element_type=f32)
    up_val = jnp.dot(normed, w_up, preferred_element_type=f32)
    hidden = (jax.nn.silu(gate_val) * up_val).astype(bf16)
    terms = jnp.dot(hidden, w_down, preferred_element_type=f32)

    terms = terms.reshape(rows, kv_count, 2, cols).transpose(2, 1, 0, 3)
    terms = jnp.concatenate([terms[:, :, :half], terms[:, :, half:]], axis=3)
    mine = lax.dynamic_index_in_dim(terms, core, 0, keepdims=False)
    theirs = lax.dynamic_index_in_dim(terms, 1 - core, 0, keepdims=False).astype(bf16)
    chip_sum = (mine + lax.ppermute(theirs, "tp", SWAP).astype(f32)).astype(bf16)
    down = jnp.sum(exchanged(chip_sum, KV).astype(f32), axis=0)
    down = jnp.concatenate([down[:, :cols], down[:, cols:]], axis=0)
    result = (mixed.astype(f32) + down).astype(bf16)
    return (result, new_state[None])


def solution(mesh):
    torus = Mesh(
        mesh.devices.reshape(mesh.shape["dp"], 8, 4, mesh.shape["tp"]), ("dp", "kv_0", "kv_1", "tp")
    )
    in_specs = (
        P("dp", KV_TP),
        P(DP_KV, "tp", None, None),
        P(),
        P(KV, "tp"),
        P(KV, "tp"),
        P(KV, "tp"),
        P(KV, "tp"),
        P("tp"),
        P("tp"),
        P(None, KV_TP),
        P(),
        P(None, KV_TP),
        P(None, KV_TP),
        P(KV_TP, None),
    )
    out_specs = (P("dp", KV_TP), P(DP_KV, "tp", None, None))
    return jax.shard_map(local, mesh=torus, in_specs=in_specs, out_specs=out_specs, check_vma=False)
```

```python
import jax
import jax.numpy as jnp
from jax import lax
from jax.experimental import pallas as pl
from jax.experimental.pallas import tpu as pltpu
from jax.sharding import Mesh
from jax.sharding import PartitionSpec as P

LANES = 128
KV = ("kv_0", "kv_1")
KV_TP = ("kv_0", "kv_1", "tp")
DP_KV = ("dp", "kv_0", "kv_1")
SWAP = [(0, 1), (1, 0)]
NT = (((1,), (1,)), ((), ()))

epsilon = 1e-06
bf16, f32 = jnp.bfloat16, jnp.float32


def exchanged(pieces, axis):
    return lax.all_to_all(pieces, axis, split_axis=0, concat_axis=0, tiled=True)


def lanes_below(core, shape):
    lane = lax.broadcasted_iota(jnp.int32, shape, len(shape) - 1)
    return (lane < LANES // 2) == (core == 0)


def half_turn(x):
    return pltpu.roll(x, LANES // 2, axis=x.ndim - 1)


def in_vmem(count):
    return [pl.BlockSpec(memory_space=pltpu.VMEM)] * count


IN_SMEM = pl.BlockSpec(memory_space=pltpu.SMEM)


def project_kernel(where, own, other, gain, wq, wf, wi, wg, out, rows_scr):
    kv, core = where[0], where[1]
    rows = own.shape[0]
    pair = jnp.concatenate([own[...].astype(f32), other[...].astype(f32)], axis=1)
    block = jnp.where(core == 0, pair, half_turn(pair))
    squares = jnp.sum(block * block, axis=1, keepdims=True)
    high = squares.astype(bf16).astype(f32)
    lane = lax.broadcasted_iota(jnp.int32, (rows, LANES), 1)
    extra = jnp.where(lane == 0, high, jnp.where(lane == 1, squares - high, 0.0))
    scaled = (block * gain[pl.ds(kv, 1), :]).astype(bf16)
    heads = wq.shape[1] // LANES
    step = out.shape[1]
    for index, weight in enumerate((wq, wf, wi, wg)):
        part = jnp.dot(scaled, weight[...], preferred_element_type=f32)
        for head in range(heads):
            rows_scr[pl.ds(index * heads + head, rows, stride=step), :] = part[
                :, head * LANES : (head + 1) * LANES
            ]
    for row in range(4 * heads, step):
        rows_scr[pl.ds(row, rows, stride=step), :] = extra
    for row in range(rows):
        out[row] = rows_scr[pl.ds(row * step, step), :].astype(bf16)


def recur_kernel(pieces, state, bound, gain, gated, forget_out, value_out, width):
    heads = state.shape[0]
    total = jnp.sum(pieces[...].astype(f32), axis=0)
    squares = total[4 * heads : 4 * heads + 1, 0:1] + total[4 * heads : 4 * heads + 1, 1:2]
    row_scale = lax.rsqrt(squares / width + epsilon)
    query_pre, forget_pre, value_in, gate_pre = [
        row_scale * total[i * heads : (i + 1) * heads] for i in range(4)
    ]
    forget = bound[...] + (1.0 - bound[...]) * jax.nn.sigmoid(forget_pre)
    key_in = 1.0 - forget
    query_act = jax.nn.silu(query_pre)
    forget_out[...] = forget
    value_out[...] = value_in
    fresh = jnp.sum(query_act * key_in, axis=1, keepdims=True) * value_in
    reads = jnp.transpose(query_act * forget)
    kept = jnp.concatenate(
        [
            jnp.sum(reads[:, head : head + 1] * state[head], axis=0, keepdims=True)
            for head in range(heads)
        ],
        axis=0,
    )
    head_out = kept + fresh
    head_out = head_out * lax.rsqrt(
        jnp.mean(head_out * head_out, axis=1, keepdims=True) + epsilon
    )
    value = (head_out * gain[...] * jax.nn.silu(gate_pre)).astype(bf16)
    for peer in range(gated.shape[0]):
        gated[peer] = value


def mix_kernel(where, every, tokens, weight, out, rows_scr, whole_scr):
    core = where[1]
    rows = tokens.shape[0]
    peers, heads, _ = every.shape
    per_row = peers * heads // rows
    rows_scr[...] = every[...].astype(f32).reshape(peers * heads, LANES)
    for head in range(per_row):
        whole_scr[:, head * LANES : (head + 1) * LANES] = rows_scr[
            pl.ds(head, rows, stride=per_row), :
        ].astype(bf16)
    added = lax.dot_general(whole_scr[...], weight[...], NT, preferred_element_type=f32)
    mixed = tokens[...].astype(f32) + added
    half = rows // 2
    packed = jnp.concatenate([mixed[:half], mixed[half:]], axis=1)
    packed = jnp.where(core == 0, packed, half_turn(packed)).astype(bf16)
    for peer in range(out.shape[0]):
        out[peer] = packed


def feed_kernel(where, own, other, gain, w_gate, w_up, w_down, mine, theirs, scr):
    core = where[1]
    blocks, half, _ = own.shape
    rows = 2 * half
    mask = lanes_below(core, (half, LANES))
    squares = jnp.zeros((rows, LANES), f32)
    for block in range(blocks):
        a, b = own[block].astype(f32), other[block].astype(f32)
        top = jnp.where(mask, a, b)
        bottom = half_turn(jnp.where(mask, b, a))
        value = jnp.concatenate([top, bottom], axis=0)
        squares = squares + value * value
        scr[:, block * LANES : (block + 1) * LANES] = (value * gain[pl.ds(block, 1), :]).astype(bf16)
    mean = jnp.sum(squares, axis=1, keepdims=True) / (blocks * LANES)
    scale = lax.rsqrt(mean + epsilon)
    normed = scr[...]
    gate = scale * lax.dot_general(normed, w_gate[...], NT, preferred_element_type=f32)
    up = scale * lax.dot_general(normed, w_up[...], NT, preferred_element_type=f32)
    hidden = (jax.nn.silu(gate) * up).astype(bf16)
    terms = jnp.dot(hidden, w_down[...], preferred_element_type=f32)
    for block in range(blocks):
        term = terms[:, block * LANES : (block + 1) * LANES]
        top, bottom = term[:half], half_turn(term[half:])
        mine[block] = jnp.where(mask, top, bottom)
        theirs[block] = jnp.where(mask, bottom, top).astype(bf16)


def sum_kernel(mine, theirs, out):
    out[...] = (mine[...] + theirs[...].astype(f32)).astype(bf16)


def finish_kernel(where, pieces, mixed, out):
    core = where[1]
    half = mixed.shape[1]
    total = mixed[0].astype(f32) + jnp.sum(pieces[...].astype(f32), axis=0)
    total = jnp.where(core == 0, total, half_turn(total))
    out[:half] = total[:, : LANES // 2].astype(bf16)
    out[half:] = half_turn(total)[:, : LANES // 2].astype(bf16)


def local(
    tokens,
    rec_state,
    norm_gain,
    w_query,
    w_forget,
    w_input,
    w_outgate,
    lower_bound,
    head_gain,
    w_heads_out,
    mixer_gain,
    w_gate,
    w_up,
    w_down,
):
    kv_count = lax.axis_size(KV)
    where = jnp.stack([lax.axis_index(KV), lax.axis_index("tp")]).astype(jnp.int32)
    rows, cols = tokens.shape
    width = norm_gain.shape[0]
    heads = rec_state.shape[1]
    half = rows // 2
    blocks = width // LANES
    shape = jax.ShapeDtypeStruct
    piece_rows = 5 * heads

    other = lax.ppermute(tokens, "tp", SWAP)
    pieces = pl.pallas_call(
        project_kernel,
        out_shape=shape((rows, piece_rows, LANES), bf16),
        in_specs=[IN_SMEM] + in_vmem(7),
        out_specs=in_vmem(1)[0],
        scratch_shapes=[pltpu.VMEM((rows * piece_rows, LANES), f32)],
        name="project",
    )(where, tokens, other, norm_gain.reshape(blocks, LANES), w_query, w_forget, w_input, w_outgate)
    pieces = exchanged(pieces, KV)

    per_head = shape((heads, LANES), f32)
    gated, forget, value_in = pl.pallas_call(
        lambda *refs: recur_kernel(*refs, width),
        out_shape=(shape((2 * kv_count, heads, LANES), bf16), per_head, per_head),
        in_specs=in_vmem(4),
        out_specs=tuple(in_vmem(3)),
        name="recur",
    )(pieces, rec_state[0], lower_bound.reshape(heads, LANES), head_gain.reshape(heads, LANES))
    new_state = forget[:, :, None] * rec_state[0] + (1.0 - forget)[:, :, None] * value_in[:, None, :]

    every = exchanged(gated, KV_TP)
    mixed = pl.pallas_call(
        mix_kernel,
        out_shape=shape((kv_count, half, LANES), bf16),
        in_specs=[IN_SMEM] + in_vmem(3),
        out_specs=in_vmem(1)[0],
        scratch_shapes=[
            pltpu.VMEM((2 * kv_count * heads, LANES), f32),
            pltpu.VMEM((rows, 2 * heads * LANES), bf16),
        ],
        name="mix",
    )(where, every, tokens, w_heads_out.T)

    own = exchanged(mixed, KV)
    other = lax.ppermute(own, "tp", SWAP)
    mine, theirs = pl.pallas_call(
        feed_kernel,
        out_shape=(shape((kv_count, half, LANES), f32), shape((kv_count, half, LANES), bf16)),
        in_specs=[IN_SMEM] + in_vmem(6),
        out_specs=tuple(in_vmem(2)),
        scratch_shapes=[pltpu.VMEM((rows, width), bf16)],
        name="feed",
    )(where, own, other, mixer_gain.reshape(blocks, LANES), w_gate.T, w_up.T, w_down)
    theirs = lax.ppermute(theirs, "tp", SWAP)
    chip_sum = pl.pallas_call(
        sum_kernel,
        out_shape=shape((kv_count, half, LANES), bf16),
        in_specs=in_vmem(2),
        out_specs=in_vmem(1)[0],
        name="chip_sum",
    )(mine, theirs)
    down = exchanged(chip_sum, KV)
    result = pl.pallas_call(
        finish_kernel,
        out_shape=shape((rows, cols), bf16),
        in_specs=[IN_SMEM] + in_vmem(2),
        out_specs=in_vmem(1)[0],
        name="finish",
    )(where, down, mixed)
    return (result, new_state[None])


def solution(mesh):
    torus = Mesh(
        mesh.devices.reshape(mesh.shape["dp"], 8, 4, mesh.shape["tp"]), ("dp", "kv_0", "kv_1", "tp")
    )
    in_specs = (
        P("dp", KV_TP),
        P(DP_KV, "tp", None, None),
        P(),
        P(KV, "tp"),
        P(KV, "tp"),
        P(KV, "tp"),
        P(KV, "tp"),
        P("tp"),
        P("tp"),
        P(None, KV_TP),
        P(),
        P(None, KV_TP),
        P(None, KV_TP),
        P(KV_TP, None),
    )
    out_specs = (P("dp", KV_TP), P(DP_KV, "tp", None, None))
    return jax.shard_map(local, mesh=torus, in_specs=in_specs, out_specs=out_specs, check_vma=False)
```

```python
import jax
import jax.numpy as jnp
from jax import lax
from jax.experimental import pallas as pl
from jax.experimental.pallas import tpu as pltpu
from jax.sharding import Mesh
from jax.sharding import PartitionSpec as P

LANES = 128
KV = ("kv_0", "kv_1")
KV_TP = ("kv_0", "kv_1", "tp")
DP_KV = ("dp", "kv_0", "kv_1")
SWAP = [(0, 1), (1, 0)]
NT = (((1,), (1,)), ((), ()))

epsilon = 1e-06
bf16, f32 = jnp.bfloat16, jnp.float32


def exchanged(pieces, axis):
    return lax.all_to_all(pieces, axis, split_axis=0, concat_axis=0, tiled=True)


def lanes_below(core, shape):
    lane = lax.broadcasted_iota(jnp.int32, shape, len(shape) - 1)
    return (lane < LANES // 2) == (core == 0)


def half_turn(x):
    return pltpu.roll(x, LANES // 2, axis=x.ndim - 1)


def in_vmem(count):
    return [pl.BlockSpec(memory_space=pltpu.VMEM)] * count


def held(*arrays):
    return [pltpu.with_memory_space_constraint(array, pltpu.VMEM) for array in arrays]


def far(*arrays):
    return [pltpu.with_memory_space_constraint(array, pltpu.HBM) for array in arrays]


LIMIT = pltpu.CompilerParams(vmem_limit_bytes=8 * 1024 * 1024)
IN_HBM = pl.BlockSpec(memory_space=pltpu.HBM)


def load_kernel(*refs):
    count = len(refs) // 2
    sources, targets, sems = refs[:count], refs[count : 2 * count], refs[-1]
    copies = [
        pltpu.make_async_copy(source, target, sems.at[index])
        for index, (source, target) in enumerate(zip(sources, targets))
    ]
    for copy in copies:
        copy.start()
    for copy in copies:
        copy.wait()


def project_kernel(own, other, gain, wq, wf, wi, wg, out, rows_scr):
    kv, core = lax.axis_index(KV), lax.axis_index("tp")
    rows = own.shape[0]
    pair = jnp.concatenate([own[...].astype(f32), other[...].astype(f32)], axis=1)
    block = jnp.where(core == 0, pair, half_turn(pair))
    squares = jnp.sum(block * block, axis=1, keepdims=True)
    high = squares.astype(bf16).astype(f32)
    lane = lax.broadcasted_iota(jnp.int32, (rows, LANES), 1)
    extra = jnp.where(lane == 0, high, jnp.where(lane == 1, squares - high, 0.0))
    scaled = (block * gain[pl.ds(kv, 1), :]).astype(bf16)
    heads = wq.shape[1] // LANES
    step = out.shape[1]
    for index, weight in enumerate((wq, wf, wi, wg)):
        part = jnp.dot(scaled, weight[...], preferred_element_type=f32)
        for head in range(heads):
            rows_scr[pl.ds(index * heads + head, rows, stride=step), :] = part[
                :, head * LANES : (head + 1) * LANES
            ]
    for row in range(4 * heads, step):
        rows_scr[pl.ds(row, rows, stride=step), :] = extra
    for row in range(rows):
        out[row] = rows_scr[pl.ds(row * step, step), :].astype(bf16)


def recur_kernel(pieces, state, bound, gain, gated, forget_out, value_out, width):
    heads = state.shape[0]
    total = jnp.sum(pieces[...].astype(f32), axis=0)
    squares = total[4 * heads : 4 * heads + 1, 0:1] + total[4 * heads : 4 * heads + 1, 1:2]
    row_scale = lax.rsqrt(squares / width + epsilon)
    query_pre, forget_pre, value_in, gate_pre = [
        row_scale * total[i * heads : (i + 1) * heads] for i in range(4)
    ]
    forget = bound[...] + (1.0 - bound[...]) * jax.nn.sigmoid(forget_pre)
    key_in = 1.0 - forget
    query_act = jax.nn.silu(query_pre)
    forget_out[...] = forget
    value_out[...] = value_in
    fresh = jnp.sum(query_act * key_in, axis=1, keepdims=True) * value_in
    reads = jnp.transpose(query_act * forget)
    kept = jnp.concatenate(
        [
            jnp.sum(reads[:, head : head + 1] * state[head], axis=0, keepdims=True)
            for head in range(heads)
        ],
        axis=0,
    )
    head_out = kept + fresh
    head_out = head_out * lax.rsqrt(
        jnp.mean(head_out * head_out, axis=1, keepdims=True) + epsilon
    )
    value = (head_out * gain[...] * jax.nn.silu(gate_pre)).astype(bf16)
    for peer in range(gated.shape[0]):
        gated[peer] = value


def mix_kernel(every, tokens, weight, out, rows_scr, whole_scr):
    core = lax.axis_index("tp")
    rows = tokens.shape[0]
    peers, heads, _ = every.shape
    per_row = peers * heads // rows
    rows_scr[...] = every[...].astype(f32).reshape(peers * heads, LANES)
    for head in range(per_row):
        whole_scr[:, head * LANES : (head + 1) * LANES] = rows_scr[
            pl.ds(head, rows, stride=per_row), :
        ].astype(bf16)
    added = lax.dot_general(whole_scr[...], weight[...], NT, preferred_element_type=f32)
    mixed = tokens[...].astype(f32) + added
    half = rows // 2
    packed = jnp.concatenate([mixed[:half], mixed[half:]], axis=1)
    packed = jnp.where(core == 0, packed, half_turn(packed)).astype(bf16)
    for peer in range(out.shape[0]):
        out[peer] = packed


def feed_kernel(own, other, gain, w_gate, w_up, w_down_hbm, mine, theirs, scr, w_down, sem):
    fetch = pltpu.make_async_copy(w_down_hbm, w_down, sem)
    fetch.start()
    core = lax.axis_index("tp")
    blocks, half, _ = own.shape
    rows = 2 * half
    mask = lanes_below(core, (half, LANES))
    squares = jnp.zeros((rows, LANES), f32)
    for block in range(blocks):
        a, b = own[block].astype(f32), other[block].astype(f32)
        top = jnp.where(mask, a, b)
        bottom = half_turn(jnp.where(mask, b, a))
        value = jnp.concatenate([top, bottom], axis=0)
        squares = squares + value * value
        scr[:, block * LANES : (block + 1) * LANES] = (value * gain[pl.ds(block, 1), :]).astype(bf16)
    mean = jnp.sum(squares, axis=1, keepdims=True) / (blocks * LANES)
    scale = lax.rsqrt(mean + epsilon)
    normed = scr[...]
    gate = scale * lax.dot_general(normed, w_gate[...], NT, preferred_element_type=f32)
    up = scale * lax.dot_general(normed, w_up[...], NT, preferred_element_type=f32)
    hidden = (jax.nn.silu(gate) * up).astype(bf16)
    fetch.wait()
    terms = jnp.dot(hidden, w_down[...], preferred_element_type=f32)
    for block in range(blocks):
        term = terms[:, block * LANES : (block + 1) * LANES]
        top, bottom = term[:half], half_turn(term[half:])
        mine[block] = jnp.where(mask, top, bottom)
        theirs[block] = jnp.where(mask, bottom, top).astype(bf16)


def sum_kernel(mine, theirs, out):
    out[...] = (mine[...] + theirs[...].astype(f32)).astype(bf16)


def finish_kernel(pieces, mixed, out):
    core = lax.axis_index("tp")
    half = mixed.shape[1]
    total = mixed[0].astype(f32) + jnp.sum(pieces[...].astype(f32), axis=0)
    total = jnp.where(core == 0, total, half_turn(total))
    out[:half] = total[:, : LANES // 2].astype(bf16)
    out[half:] = half_turn(total)[:, : LANES // 2].astype(bf16)


def local(
    tokens,
    rec_state,
    norm_gain,
    w_query,
    w_forget,
    w_input,
    w_outgate,
    lower_bound,
    head_gain,
    w_heads_out,
    mixer_gain,
    w_gate,
    w_up,
    w_down,
):
    kv_count = lax.axis_size(KV)
    rows, cols = tokens.shape
    width = norm_gain.shape[0]
    heads = rec_state.shape[1]
    half = rows // 2
    blocks = width // LANES
    shape = pltpu.VMEM
    piece_rows = 5 * heads

    other = lax.ppermute(tokens, "tp", SWAP)
    loads = (
        tokens,
        norm_gain.reshape(blocks, LANES),
        lower_bound.reshape(heads, LANES),
        head_gain.reshape(heads, LANES),
        mixer_gain.reshape(blocks, LANES),
        w_heads_out.T,
        w_query,
        w_forget,
        w_input,
        w_outgate,
    )
    tokens_here, first_gain, bound, gain, second_gain, heads_out, *projections = pl.pallas_call(
        load_kernel,
        out_shape=tuple(shape(x.shape, x.dtype) for x in loads),
        in_specs=[IN_HBM] * len(loads),
        out_specs=tuple(in_vmem(len(loads))),
        scratch_shapes=[pltpu.SemaphoreType.DMA((len(loads),))],
        compiler_params=LIMIT,
        name="load",
    )(*far(*loads))
    pieces = pl.pallas_call(
        project_kernel,
        out_shape=shape((rows, piece_rows, LANES), bf16),
        in_specs=in_vmem(7),
        out_specs=in_vmem(1)[0],
        scratch_shapes=[pltpu.VMEM((rows * piece_rows, LANES), f32)],
        compiler_params=LIMIT,
        name="project",
    )(
        *held(tokens_here, other, first_gain, *projections)
    )
    pieces = exchanged(pieces, KV)

    per_head = shape((heads, LANES), f32)
    gated, forget, value_in = pl.pallas_call(
        lambda *refs: recur_kernel(*refs, width),
        out_shape=(shape((2 * kv_count, heads, LANES), bf16), per_head, per_head),
        in_specs=in_vmem(4),
        out_specs=tuple(in_vmem(3)),
        compiler_params=LIMIT,
        name="recur",
    )(*held(pieces, rec_state[0], bound, gain))
    new_state = forget[:, :, None] * rec_state[0] + (1.0 - forget)[:, :, None] * value_in[:, None, :]

    every = exchanged(gated, KV_TP)
    mixed = pl.pallas_call(
        mix_kernel,
        out_shape=shape((kv_count, half, LANES), bf16),
        in_specs=in_vmem(3),
        out_specs=in_vmem(1)[0],
        scratch_shapes=[
            pltpu.VMEM((2 * kv_count * heads, LANES), f32),
            pltpu.VMEM((rows, 2 * heads * LANES), bf16),
        ],
        compiler_params=LIMIT,
        name="mix",
    )(*held(every, tokens_here, heads_out))

    own = exchanged(mixed, KV)
    other = lax.ppermute(own, "tp", SWAP)
    mine, theirs = pl.pallas_call(
        feed_kernel,
        out_shape=(shape((kv_count, half, LANES), f32), shape((kv_count, half, LANES), bf16)),
        in_specs=in_vmem(5) + [IN_HBM],
        out_specs=tuple(in_vmem(2)),
        scratch_shapes=[
            pltpu.VMEM((rows, width), bf16),
            pltpu.VMEM(w_down.shape, bf16),
            pltpu.SemaphoreType.DMA,
        ],
        compiler_params=LIMIT,
        name="feed",
    )(
        *held(own, other, second_gain, w_gate.T, w_up.T), *far(w_down)
    )
    theirs = lax.ppermute(theirs, "tp", SWAP)
    chip_sum = pl.pallas_call(
        sum_kernel,
        out_shape=shape((kv_count, half, LANES), bf16),
        in_specs=in_vmem(2),
        out_specs=in_vmem(1)[0],
        compiler_params=LIMIT,
        name="chip_sum",
    )(*held(mine, theirs))
    down = exchanged(chip_sum, KV)
    result = pl.pallas_call(
        finish_kernel,
        out_shape=jax.ShapeDtypeStruct((rows, cols), bf16),
        in_specs=in_vmem(2),
        out_specs=in_vmem(1)[0],
        compiler_params=LIMIT,
        name="finish",
    )(*held(down, mixed))
    return (result, new_state[None])


def solution(mesh):
    torus = Mesh(
        mesh.devices.reshape(mesh.shape["dp"], 8, 4, mesh.shape["tp"]), ("dp", "kv_0", "kv_1", "tp")
    )
    in_specs = (
        P("dp", KV_TP),
        P(DP_KV, "tp", None, None),
        P(),
        P(KV, "tp"),
        P(KV, "tp"),
        P(KV, "tp"),
        P(KV, "tp"),
        P("tp"),
        P("tp"),
        P(None, KV_TP),
        P(),
        P(None, KV_TP),
        P(None, KV_TP),
        P(KV_TP, None),
    )
    out_specs = (P("dp", KV_TP), P(DP_KV, "tp", None, None))
    return jax.shard_map(local, mesh=torus, in_specs=in_specs, out_specs=out_specs, check_vma=False)
```

```python
import jax
import jax.numpy as jnp
from jax import lax
from jax.experimental import pallas as pl
from jax.experimental.pallas import tpu as pltpu
from jax.sharding import Mesh
from jax.sharding import PartitionSpec as P

LANES = 128
KV = ("kv_0", "kv_1")
KV_TP = ("kv_0", "kv_1", "tp")
DP_KV = ("dp", "kv_0", "kv_1")
SWAP = [(0, 1), (1, 0)]
NT = (((1,), (1,)), ((), ()))

epsilon = 1e-06
bf16, f32 = jnp.bfloat16, jnp.float32


def exchanged(pieces, axis):
    return lax.all_to_all(pieces, axis, split_axis=0, concat_axis=0, tiled=True)


def lanes_below(core, shape):
    lane = lax.broadcasted_iota(jnp.int32, shape, len(shape) - 1)
    return (lane < LANES // 2) == (core == 0)


def half_turn(x):
    return pltpu.roll(x, LANES // 2, axis=x.ndim - 1)


def in_vmem(count):
    return [pl.BlockSpec(memory_space=pltpu.VMEM)] * count


def held(*arrays):
    return [pltpu.with_memory_space_constraint(array, pltpu.VMEM) for array in arrays]


def far(*arrays):
    return [pltpu.with_memory_space_constraint(array, pltpu.HBM) for array in arrays]


LIMIT = pltpu.CompilerParams(vmem_limit_bytes=8 * 1024 * 1024)
IN_HBM = pl.BlockSpec(memory_space=pltpu.HBM)


def load_kernel(*refs):
    count = len(refs) // 2
    sources, targets, sems = refs[:count], refs[count : 2 * count], refs[-1]
    copies = [
        pltpu.make_async_copy(source, target, sems.at[index])
        for index, (source, target) in enumerate(zip(sources, targets))
    ]
    for copy in copies:
        copy.start()
    for copy in copies:
        copy.wait()


def project_kernel(own, other, gain, wq, wf, wi, wg, out, rows_scr):
    kv, core = lax.axis_index(KV), lax.axis_index("tp")
    rows = own.shape[0]
    pair = jnp.concatenate([own[...].astype(f32), other[...].astype(f32)], axis=1)
    block = jnp.where(core == 0, pair, half_turn(pair))
    squares = jnp.sum(block * block, axis=1, keepdims=True)
    high = squares.astype(bf16).astype(f32)
    lane = lax.broadcasted_iota(jnp.int32, (rows, LANES), 1)
    extra = jnp.where(lane == 0, high, jnp.where(lane == 1, squares - high, 0.0))
    scaled = (block * gain[pl.ds(kv, 1), :]).astype(bf16)
    heads = wq.shape[1] // LANES
    step = out.shape[1]
    for index, weight in enumerate((wq, wf, wi, wg)):
        part = jnp.dot(scaled, weight[...], preferred_element_type=f32)
        for head in range(heads):
            rows_scr[pl.ds(index * heads + head, rows, stride=step), :] = part[
                :, head * LANES : (head + 1) * LANES
            ]
    for row in range(4 * heads, step):
        rows_scr[pl.ds(row, rows, stride=step), :] = extra
    for row in range(rows):
        out[row] = rows_scr[pl.ds(row * step, step), :].astype(bf16)


def recur_kernel(pieces, state, bound, gain, gated, new_state, width):
    heads = state.shape[0]
    total = jnp.sum(pieces[...].astype(f32), axis=0)
    squares = total[4 * heads : 4 * heads + 1, 0:1] + total[4 * heads : 4 * heads + 1, 1:2]
    row_scale = lax.rsqrt(squares / width + epsilon)
    query_pre, forget_pre, value_in, gate_pre = [
        row_scale * total[i * heads : (i + 1) * heads] for i in range(4)
    ]
    forget = bound[...] + (1.0 - bound[...]) * jax.nn.sigmoid(forget_pre)
    forget_down = jnp.transpose(forget)
    query_down = jnp.transpose(jax.nn.silu(query_pre))
    reads = []
    for head in range(heads):
        keep = jnp.broadcast_to(forget_down[:, head : head + 1], state.shape[1:])
        fresh = keep * state[head] + (1.0 - keep) * value_in[head : head + 1]
        new_state[head] = fresh
        reads.append(jnp.sum(query_down[:, head : head + 1] * fresh, axis=0, keepdims=True))
    head_out = jnp.concatenate(reads, axis=0)
    head_out = head_out * lax.rsqrt(
        jnp.mean(head_out * head_out, axis=1, keepdims=True) + epsilon
    )
    value = (head_out * gain[...] * jax.nn.silu(gate_pre)).astype(bf16)
    for peer in range(gated.shape[0]):
        gated[peer] = value


def mix_kernel(own, other, tokens, weight, out, rows_scr, whole_scr):
    core = lax.axis_index("tp")
    rows = tokens.shape[0]
    heads = own.shape[1]
    rows_scr[0] = own[...].astype(f32).reshape(rows * heads, LANES)
    rows_scr[1] = other[...].astype(f32).reshape(rows * heads, LANES)
    for side in range(2):
        source = (core + side) % 2
        for head in range(heads):
            column = (side * heads + head) * LANES
            whole_scr[:, column : column + LANES] = rows_scr[
                source, pl.ds(head, rows, stride=heads), :
            ].astype(bf16)
    added = lax.dot_general(whole_scr[...], weight[...], NT, preferred_element_type=f32)
    mixed = tokens[...].astype(f32) + added
    half = rows // 2
    packed = jnp.concatenate([mixed[:half], mixed[half:]], axis=1)
    packed = jnp.where(core == 0, packed, half_turn(packed)).astype(bf16)
    for peer in range(out.shape[0]):
        out[peer] = packed


def feed_kernel(
    own, other, gain, w_gate, w_up, state, w_down_hbm, mine, theirs, state_hbm, scr, w_down, sems
):
    fetch = pltpu.make_async_copy(w_down_hbm, w_down, sems.at[0])
    fetch.start()
    store = pltpu.make_async_copy(state, state_hbm, sems.at[1])
    store.start()
    core = lax.axis_index("tp")
    blocks, half, _ = own.shape
    rows = 2 * half
    mask = lanes_below(core, (half, LANES))
    squares = jnp.zeros((rows, LANES), f32)
    for block in range(blocks):
        a, b = own[block].astype(f32), other[block].astype(f32)
        top = jnp.where(mask, a, b)
        bottom = half_turn(jnp.where(mask, b, a))
        value = jnp.concatenate([top, bottom], axis=0)
        squares = squares + value * value
        scr[:, block * LANES : (block + 1) * LANES] = (value * gain[pl.ds(block, 1), :]).astype(bf16)
    mean = jnp.sum(squares, axis=1, keepdims=True) / (blocks * LANES)
    scale = lax.rsqrt(mean + epsilon)
    normed = scr[...]
    gate = scale * lax.dot_general(normed, w_gate[...], NT, preferred_element_type=f32)
    up = scale * lax.dot_general(normed, w_up[...], NT, preferred_element_type=f32)
    hidden = (jax.nn.silu(gate) * up).astype(bf16)
    fetch.wait()
    terms = jnp.dot(hidden, w_down[...], preferred_element_type=f32)
    for block in range(blocks):
        term = terms[:, block * LANES : (block + 1) * LANES]
        top, bottom = term[:half], half_turn(term[half:])
        mine[block] = jnp.where(mask, top, bottom)
        theirs[block] = jnp.where(mask, bottom, top).astype(bf16)
    store.wait()


def sum_kernel(mine, theirs, out):
    out[...] = (mine[...] + theirs[...].astype(f32)).astype(bf16)


def finish_kernel(pieces, mixed, out):
    core = lax.axis_index("tp")
    half = mixed.shape[1]
    total = mixed[0].astype(f32) + jnp.sum(pieces[...].astype(f32), axis=0)
    total = jnp.where(core == 0, total, half_turn(total))
    out[:half] = total[:, : LANES // 2].astype(bf16)
    out[half:] = half_turn(total)[:, : LANES // 2].astype(bf16)


def local(
    tokens,
    rec_state,
    norm_gain,
    w_query,
    w_forget,
    w_input,
    w_outgate,
    lower_bound,
    head_gain,
    w_heads_out,
    mixer_gain,
    w_gate,
    w_up,
    w_down,
):
    kv_count = lax.axis_size(KV)
    rows, cols = tokens.shape
    width = norm_gain.shape[0]
    heads = rec_state.shape[1]
    half = rows // 2
    blocks = width // LANES
    shape = pltpu.VMEM
    piece_rows = 5 * heads

    other = lax.ppermute(tokens, "tp", SWAP)
    loads = (
        tokens,
        norm_gain.reshape(blocks, LANES),
        lower_bound.reshape(heads, LANES),
        head_gain.reshape(heads, LANES),
        mixer_gain.reshape(blocks, LANES),
        w_heads_out.T,
        w_query,
        w_forget,
        w_input,
        w_outgate,
    )
    tokens_here, first_gain, bound, gain, second_gain, heads_out, *projections = pl.pallas_call(
        load_kernel,
        out_shape=tuple(shape(x.shape, x.dtype) for x in loads),
        in_specs=[IN_HBM] * len(loads),
        out_specs=tuple(in_vmem(len(loads))),
        scratch_shapes=[pltpu.SemaphoreType.DMA((len(loads),))],
        compiler_params=LIMIT,
        name="load",
    )(*far(*loads))
    pieces = pl.pallas_call(
        project_kernel,
        out_shape=shape((rows, piece_rows, LANES), bf16),
        in_specs=in_vmem(7),
        out_specs=in_vmem(1)[0],
        scratch_shapes=[pltpu.VMEM((rows * piece_rows, LANES), f32)],
        compiler_params=LIMIT,
        name="project",
    )(
        *held(tokens_here, other, first_gain, *projections)
    )
    pieces = exchanged(pieces, KV)

    gated, new_state = pl.pallas_call(
        lambda *refs: recur_kernel(*refs, width),
        out_shape=(shape((kv_count, heads, LANES), bf16), shape(rec_state.shape[1:], f32)),
        in_specs=in_vmem(4),
        out_specs=tuple(in_vmem(2)),
        compiler_params=LIMIT,
        name="recur",
    )(*held(pieces, rec_state[0], bound, gain))

    own = exchanged(gated, KV)
    other = lax.ppermute(own, "tp", SWAP)
    mixed = pl.pallas_call(
        mix_kernel,
        out_shape=shape((kv_count, half, LANES), bf16),
        in_specs=in_vmem(4),
        out_specs=in_vmem(1)[0],
        scratch_shapes=[
            pltpu.VMEM((2, rows * heads, LANES), f32),
            pltpu.VMEM((rows, 2 * heads * LANES), bf16),
        ],
        compiler_params=LIMIT,
        name="mix",
    )(*held(own, other, tokens_here, heads_out))

    own = exchanged(mixed, KV)
    other = lax.ppermute(own, "tp", SWAP)
    mine, theirs, new_state = pl.pallas_call(
        feed_kernel,
        out_shape=(
            shape((kv_count, half, LANES), f32),
            shape((kv_count, half, LANES), bf16),
            pltpu.HBM(new_state.shape, f32),
        ),
        in_specs=in_vmem(6) + [IN_HBM],
        out_specs=tuple(in_vmem(2) + [IN_HBM]),
        scratch_shapes=[
            pltpu.VMEM((rows, width), bf16),
            pltpu.VMEM(w_down.shape, bf16),
            pltpu.SemaphoreType.DMA((2,)),
        ],
        compiler_params=LIMIT,
        name="feed",
    )(
        *held(own, other, second_gain, w_gate.T, w_up.T, new_state), *far(w_down)
    )
    theirs = lax.ppermute(theirs, "tp", SWAP)
    chip_sum = pl.pallas_call(
        sum_kernel,
        out_shape=shape((kv_count, half, LANES), bf16),
        in_specs=in_vmem(2),
        out_specs=in_vmem(1)[0],
        compiler_params=LIMIT,
        name="chip_sum",
    )(*held(mine, theirs))
    down = exchanged(chip_sum, KV)
    result = pl.pallas_call(
        finish_kernel,
        out_shape=jax.ShapeDtypeStruct((rows, cols), bf16),
        in_specs=in_vmem(2),
        out_specs=in_vmem(1)[0],
        compiler_params=LIMIT,
        name="finish",
    )(*held(down, mixed))
    return (result, new_state[None])


def solution(mesh):
    torus = Mesh(
        mesh.devices.reshape(mesh.shape["dp"], 8, 4, mesh.shape["tp"]), ("dp", "kv_0", "kv_1", "tp")
    )
    in_specs = (
        P("dp", KV_TP),
        P(DP_KV, "tp", None, None),
        P(),
        P(KV, "tp"),
        P(KV, "tp"),
        P(KV, "tp"),
        P(KV, "tp"),
        P("tp"),
        P("tp"),
        P(None, KV_TP),
        P(),
        P(None, KV_TP),
        P(None, KV_TP),
        P(KV_TP, None),
    )
    out_specs = (P("dp", KV_TP), P(DP_KV, "tp", None, None))
    return jax.shard_map(local, mesh=torus, in_specs=in_specs, out_specs=out_specs, check_vma=False)
```

```python
import jax
import jax.numpy as jnp
from jax import lax
from jax.experimental import pallas as pl
from jax.experimental.pallas import tpu as pltpu
from jax.sharding import Mesh
from jax.sharding import PartitionSpec as P

LANES = 128
KV = ("kv_0", "kv_1")
KV_TP = ("kv_0", "kv_1", "tp")
DP_KV = ("dp", "kv_0", "kv_1")
SWAP = [(0, 1), (1, 0)]
NT = (((1,), (1,)), ((), ()))

epsilon = 1e-06
bf16, f32 = jnp.bfloat16, jnp.float32


def exchanged(pieces, axis):
    return lax.all_to_all(pieces, axis, split_axis=0, concat_axis=0, tiled=True)


def low_lanes(shape):
    return lax.broadcasted_iota(jnp.int32, shape, len(shape) - 1) < LANES // 2


def half_turn(x):
    return pltpu.roll(x, LANES // 2, axis=x.ndim - 1)


def in_vmem(count):
    return [pl.BlockSpec(memory_space=pltpu.VMEM)] * count


def held(*arrays):
    return [pltpu.with_memory_space_constraint(array, pltpu.VMEM) for array in arrays]


def far(*arrays):
    return [pltpu.with_memory_space_constraint(array, pltpu.HBM) for array in arrays]


LIMIT = pltpu.CompilerParams(vmem_limit_bytes=8 * 1024 * 1024)
IN_HBM = pl.BlockSpec(memory_space=pltpu.HBM)


def load_kernel(*refs):
    count = len(refs) // 2
    sources, targets, sems = refs[:count], refs[count : 2 * count], refs[-1]
    copies = [
        pltpu.make_async_copy(source, target, sems.at[index])
        for index, (source, target) in enumerate(zip(sources, targets))
    ]
    for copy in copies:
        copy.start()
    for copy in copies:
        copy.wait()


def project_kernel(own, other, gain, wq, wf, wi, wg, out, rows_scr):
    kv, core = lax.axis_index(KV), lax.axis_index("tp")
    rows = own.shape[0]
    pair = jnp.concatenate([own[...].astype(f32), other[...].astype(f32)], axis=1)
    block = jnp.where(core == 0, pair, half_turn(pair))
    squares = jnp.sum(block * block, axis=1, keepdims=True)
    high = squares.astype(bf16).astype(f32)
    lane = lax.broadcasted_iota(jnp.int32, (rows, LANES), 1)
    extra = jnp.where(lane == 0, high, jnp.where(lane == 1, squares - high, 0.0))
    scaled = (block * gain[pl.ds(kv, 1), :]).astype(bf16)
    heads = wq.shape[1] // LANES
    step = out.shape[1] * out.shape[2]
    for index, weight in enumerate((wq, wf, wi, wg)):
        part = jnp.dot(scaled, weight[...], preferred_element_type=f32)
        for head in range(heads):
            rows_scr[pl.ds(index * heads + head, rows, stride=step), :] = part[
                :, head * LANES : (head + 1) * LANES
            ]
    for row in range(4 * heads, step):
        rows_scr[pl.ds(row, rows, stride=step), :] = extra
    for row in range(rows):
        piece = rows_scr[pl.ds(row * step, step), :].reshape(out.shape[1:])
        out[row] = piece.astype(bf16)


def recur_kernel(pieces, state, bound, gain, gated, new_state, width):
    heads = state.shape[0]
    total = jnp.sum(pieces[...].astype(f32), axis=0)
    total = total.reshape(total.shape[0] * total.shape[1], LANES)
    squares = total[4 * heads : 4 * heads + 1, 0:1] + total[4 * heads : 4 * heads + 1, 1:2]
    row_scale = lax.rsqrt(squares / width + epsilon)
    query_pre, forget_pre, value_in, gate_pre = [
        row_scale * total[i * heads : (i + 1) * heads] for i in range(4)
    ]
    forget = bound[...] + (1.0 - bound[...]) * jax.nn.sigmoid(forget_pre)
    forget_down = jnp.transpose(forget)
    query_down = jnp.transpose(jax.nn.silu(query_pre))
    reads = []
    for head in range(heads):
        keep = jnp.broadcast_to(forget_down[:, head : head + 1], state.shape[1:])
        fresh = keep * state[head] + (1.0 - keep) * value_in[head : head + 1]
        new_state[head] = fresh
        reads.append(jnp.sum(query_down[:, head : head + 1] * fresh, axis=0, keepdims=True))
    head_out = jnp.concatenate(reads, axis=0)
    head_out = head_out * lax.rsqrt(
        jnp.mean(head_out * head_out, axis=1, keepdims=True) + epsilon
    )
    value = (head_out * gain[...] * jax.nn.silu(gate_pre)).astype(bf16)
    for peer in range(gated.shape[0]):
        gated[peer] = value


def mix_kernel(own, other, tokens, weight, out, rows_scr, whole_scr):
    core = lax.axis_index("tp")
    rows = tokens.shape[0]
    heads = own.shape[1]
    rows_scr[0] = own[...].astype(f32).reshape(rows * heads, LANES)
    rows_scr[1] = other[...].astype(f32).reshape(rows * heads, LANES)
    for side in range(2):
        source = (core + side) % 2
        for head in range(heads):
            column = (side * heads + head) * LANES
            whole_scr[:, column : column + LANES] = rows_scr[
                source, pl.ds(head, rows, stride=heads), :
            ].astype(bf16)
    added = lax.dot_general(whole_scr[...], weight[...], NT, preferred_element_type=f32)
    mixed = tokens[...].astype(f32) + added
    half = rows // 2
    packed = jnp.concatenate([mixed[:half], mixed[half:]], axis=1)
    packed = jnp.where(core == 0, packed, half_turn(packed)).astype(bf16)
    for peer in range(out.shape[0]):
        out[peer] = packed


def part(index):
    return slice(index * LANES, (index + 1) * LANES)


def split_lanes(low, left, right):
    return jnp.where(low, left, half_turn(right)), jnp.where(low, half_turn(left), right)


def arrange_in_kernel(w_gate, w_up, gain, ins, gains):
    units = w_gate.shape[0]
    low = low_lanes((units, LANES))
    for pair in range(w_gate.shape[1] // (2 * LANES)):
        left, right = part(2 * pair), part(2 * pair + 1)
        for index, weight in enumerate((w_gate, w_up)):
            first, second = split_lanes(low, weight[:, left], weight[:, right])
            ins[0, index * units : (index + 1) * units, part(pair)] = first
            ins[1, index * units : (index + 1) * units, part(pair)] = second
        first, second = split_lanes(
            low[:1], gain[2 * pair : 2 * pair + 1, :], gain[2 * pair + 1 : 2 * pair + 2, :]
        )
        gains[0, pair : pair + 1, :] = first
        gains[1, pair : pair + 1, :] = second


def arrange_out_kernel(w_down, outs):
    low = low_lanes((w_down.shape[0], LANES))
    for pair in range(w_down.shape[1] // (2 * LANES)):
        first, second = split_lanes(low, w_down[:, part(2 * pair)], w_down[:, part(2 * pair + 1)])
        outs[0, :, part(pair)] = first
        outs[1, :, part(pair)] = second


def half_feed(core, chunk, gains, ins, scr):
    blocks, half, _ = chunk.shape
    low = low_lanes((half, LANES))
    squares = jnp.zeros((2 * half, LANES), f32)
    for pair in range(blocks // 2):
        first, second = split_lanes(
            low, chunk[2 * pair].astype(f32), chunk[2 * pair + 1].astype(f32)
        )
        value = jnp.concatenate([first, second], axis=0)
        squares = squares + value * value
        scr[:, part(pair)] = (value * gains[core, pair : pair + 1, :]).astype(bf16)
    products = lax.dot_general(scr[...], ins[core], NT, preferred_element_type=f32)
    return products, squares


def own_kernel(chunk, gains, ins, products, squares, scr):
    products[...], squares[...] = half_feed(lax.axis_index("tp"), chunk, gains, ins, scr)


def packed_rows(low, block, turned):
    half = block.shape[0] // 2
    first, second = block[:half], block[half:]
    if turned:
        first, second = second, first
    return split_lanes(low, first, second)


def other_kernel(
    chunk, gains, ins, products, squares, outs, state, theirs, hidden_out, state_hbm, scr, sem
):
    store = pltpu.make_async_copy(state, state_hbm, sem)
    store.start()
    core = lax.axis_index("tp")
    half = chunk.shape[1]
    more, more_squares = half_feed(1 - core, chunk, gains, ins, scr)
    totals = products[...] + jnp.concatenate([more[half:], more[:half]], axis=0)
    both = squares[...] + jnp.concatenate([more_squares[half:], more_squares[:half]], axis=0)
    mean = jnp.sum(both, axis=1, keepdims=True) / (chunk.shape[0] * LANES)
    totals = totals * lax.rsqrt(mean + epsilon)
    units = totals.shape[1] // 2
    hidden = (jax.nn.silu(totals[:, :units]) * totals[:, units:]).astype(bf16)
    hidden_out[...] = hidden
    terms = jnp.dot(hidden, outs[1 - core], preferred_element_type=f32)
    low = low_lanes((half, LANES))
    for pair in range(chunk.shape[0] // 2):
        left, right = packed_rows(low, terms[:, part(pair)], True)
        theirs[2 * pair] = left.astype(bf16)
        theirs[2 * pair + 1] = right.astype(bf16)
    store.wait()


def mine_kernel(hidden, outs, mine):
    terms = jnp.dot(hidden[...], outs[lax.axis_index("tp")], preferred_element_type=f32)
    low = low_lanes(mine.shape[1:])
    for pair in range(mine.shape[0] // 2):
        mine[2 * pair], mine[2 * pair + 1] = packed_rows(low, terms[:, part(pair)], False)


def sum_kernel(mine, theirs, out):
    out[...] = (mine[...] + theirs[...].astype(f32)).astype(bf16)


def finish_kernel(pieces, mixed, out):
    core = lax.axis_index("tp")
    half = mixed.shape[1]
    total = mixed[0].astype(f32) + jnp.sum(pieces[...].astype(f32), axis=0)
    total = jnp.where(core == 0, total, half_turn(total))
    out[:half] = total[:, : LANES // 2].astype(bf16)
    out[half:] = half_turn(total)[:, : LANES // 2].astype(bf16)


def local(
    tokens,
    rec_state,
    norm_gain,
    w_query,
    w_forget,
    w_input,
    w_outgate,
    lower_bound,
    head_gain,
    w_heads_out,
    mixer_gain,
    w_gate,
    w_up,
    w_down,
):
    kv_count = lax.axis_size(KV)
    rows, cols = tokens.shape
    width = norm_gain.shape[0]
    heads = rec_state.shape[1]
    half = rows // 2
    blocks = width // LANES
    shape = pltpu.VMEM
    piece_rows = 4 * heads + 4

    other = lax.ppermute(tokens, "tp", SWAP)
    loads = (
        tokens,
        norm_gain.reshape(blocks, LANES),
        lower_bound.reshape(heads, LANES),
        head_gain.reshape(heads, LANES),
        mixer_gain.reshape(blocks, LANES),
        w_heads_out.T,
    )
    tokens_here, first_gain, bound, gain, second_gain, heads_out = pl.pallas_call(
        load_kernel,
        out_shape=tuple(shape(x.shape, x.dtype) for x in loads),
        in_specs=[IN_HBM] * len(loads),
        out_specs=tuple(in_vmem(len(loads))),
        scratch_shapes=[pltpu.SemaphoreType.DMA((len(loads),))],
        compiler_params=LIMIT,
        cost_estimate=pl.CostEstimate(flops=4000000000, bytes_accessed=20000000, transcendentals=0),
        name="load",
    )(*far(*loads))
    pieces = pl.pallas_call(
        project_kernel,
        out_shape=shape((rows, piece_rows // 4, 4, LANES), bf16),
        in_specs=in_vmem(7),
        out_specs=in_vmem(1)[0],
        scratch_shapes=[pltpu.VMEM((rows * piece_rows, LANES), f32)],
        compiler_params=LIMIT,
        name="project",
    )(
        *held(tokens_here, other, first_gain, w_query, w_forget, w_input, w_outgate)
    )
    pieces = exchanged(pieces, KV)

    gated, new_state = pl.pallas_call(
        lambda *refs: recur_kernel(*refs, width),
        out_shape=(shape((kv_count, heads, LANES), bf16), shape(rec_state.shape[1:], f32)),
        in_specs=in_vmem(4),
        out_specs=tuple(in_vmem(2)),
        compiler_params=LIMIT,
        name="recur",
    )(*held(pieces, rec_state[0], bound, gain))

    own = exchanged(gated, KV)
    other = lax.ppermute(own, "tp", SWAP)
    mixed = pl.pallas_call(
        mix_kernel,
        out_shape=shape((kv_count, half, LANES), bf16),
        in_specs=in_vmem(4),
        out_specs=in_vmem(1)[0],
        scratch_shapes=[
            pltpu.VMEM((2, rows * heads, LANES), f32),
            pltpu.VMEM((rows, 2 * heads * LANES), bf16),
        ],
        compiler_params=LIMIT,
        name="mix",
    )(*held(own, other, tokens_here, heads_out))

    units = w_gate.shape[1]
    ins, gains = pl.pallas_call(
        arrange_in_kernel,
        out_shape=(
            shape((2, 2 * units, width // 2), bf16),
            shape((2, blocks // 2, LANES), f32),
        ),
        in_specs=in_vmem(3),
        out_specs=tuple(in_vmem(2)),
        compiler_params=LIMIT,
        name="arrange_in",
    )(*held(w_gate.T, w_up.T, second_gain))
    outs = pl.pallas_call(
        arrange_out_kernel,
        out_shape=shape((2, units, width // 2), bf16),
        in_specs=in_vmem(1),
        out_specs=in_vmem(1)[0],
        compiler_params=LIMIT,
        name="arrange_out",
    )(*held(w_down))

    own = exchanged(mixed, KV)
    other = lax.ppermute(own, "tp", SWAP)
    chunks = (kv_count, half, LANES)
    products, squares = pl.pallas_call(
        own_kernel,
        out_shape=(shape((rows, 2 * units), f32), shape((rows, LANES), f32)),
        in_specs=in_vmem(3),
        out_specs=tuple(in_vmem(2)),
        scratch_shapes=[pltpu.VMEM((rows, width // 2), bf16)],
        compiler_params=LIMIT,
        name="own",
    )(*held(own, gains, ins))
    theirs, hidden, new_state = pl.pallas_call(
        other_kernel,
        out_shape=(
            shape(chunks, bf16),
            shape((rows, units), bf16),
            pltpu.HBM(new_state.shape, f32),
        ),
        in_specs=in_vmem(7),
        out_specs=tuple(in_vmem(2) + [IN_HBM]),
        scratch_shapes=[pltpu.VMEM((rows, width // 2), bf16), pltpu.SemaphoreType.DMA],
        compiler_params=LIMIT,
        name="other",
    )(*held(other, gains, ins, products, squares, outs, new_state))
    mine = pl.pallas_call(
        mine_kernel,
        out_shape=shape(chunks, f32),
        in_specs=in_vmem(2),
        out_specs=in_vmem(1)[0],
        compiler_params=LIMIT,
        name="mine",
    )(*held(hidden, outs))
    theirs = lax.ppermute(theirs, "tp", SWAP)
    chip_sum = pl.pallas_call(
        sum_kernel,
        out_shape=shape((kv_count, half, LANES), bf16),
        in_specs=in_vmem(2),
        out_specs=in_vmem(1)[0],
        compiler_params=LIMIT,
        name="chip_sum",
    )(*held(mine, theirs))
    down = exchanged(chip_sum, KV)
    result = pl.pallas_call(
        finish_kernel,
        out_shape=jax.ShapeDtypeStruct((rows, cols), bf16),
        in_specs=in_vmem(2),
        out_specs=in_vmem(1)[0],
        compiler_params=LIMIT,
        name="finish",
    )(*held(down, mixed))
    return (result, new_state[None])


def solution(mesh):
    torus = Mesh(
        mesh.devices.reshape(mesh.shape["dp"], 8, 4, mesh.shape["tp"]), ("dp", "kv_0", "kv_1", "tp")
    )
    in_specs = (
        P("dp", KV_TP),
        P(DP_KV, "tp", None, None),
        P(),
        P(KV, "tp"),
        P(KV, "tp"),
        P(KV, "tp"),
        P(KV, "tp"),
        P("tp"),
        P("tp"),
        P(None, KV_TP),
        P(),
        P(None, KV_TP),
        P(None, KV_TP),
        P(KV_TP, None),
    )
    out_specs = (P("dp", KV_TP), P(DP_KV, "tp", None, None))


    return jax.shard_map(local, mesh=torus, in_specs=in_specs, out_specs=out_specs, check_vma=False)
```

```python
import jax
import jax.numpy as jnp
from jax import lax
from jax.experimental import pallas as pl
from jax.experimental.pallas import tpu as pltpu
from jax.sharding import Mesh
from jax.sharding import PartitionSpec as P

LANES = 128
KV = ("kv_0", "kv_1")
KV_TP = ("kv_0", "kv_1", "tp")
DP_KV = ("dp", "kv_0", "kv_1")
SWAP = [(0, 1), (1, 0)]
NT = (((1,), (1,)), ((), ()))

epsilon = 1e-06
bf16, f32 = jnp.bfloat16, jnp.float32


FIRST = 22
COUNT = 32
MEMBERS = [(FIRST + slot) % COUNT for slot in range(COUNT)]
SLOTS = [MEMBERS.index(place) for place in range(COUNT)]


def exchanged(pieces):
    return lax.all_to_all(
        pieces, KV, split_axis=0, concat_axis=0, axis_index_groups=[MEMBERS], tiled=True
    )


def low_lanes(shape):
    return lax.broadcasted_iota(jnp.int32, shape, len(shape) - 1) < LANES // 2


def half_turn(x):
    return pltpu.roll(x, LANES // 2, axis=x.ndim - 1)


def in_vmem(count):
    return [pl.BlockSpec(memory_space=pltpu.VMEM)] * count


def held(*arrays):
    return [pltpu.with_memory_space_constraint(array, pltpu.VMEM) for array in arrays]


def far(*arrays):
    return [pltpu.with_memory_space_constraint(array, pltpu.HBM) for array in arrays]


LIMIT = pltpu.CompilerParams(vmem_limit_bytes=8 * 1024 * 1024)
IN_HBM = pl.BlockSpec(memory_space=pltpu.HBM)


def load_kernel(*refs):
    count = len(refs) // 2
    sources, targets, sems = refs[:count], refs[count : 2 * count], refs[-1]
    copies = [
        pltpu.make_async_copy(source, target, sems.at[index])
        for index, (source, target) in enumerate(zip(sources, targets))
    ]
    for copy in copies:
        copy.start()
    for copy in copies:
        copy.wait()


def project_kernel(own, other, gain, wq, wf, wi, wg, out, rows_scr):
    kv, core = lax.axis_index(KV), lax.axis_index("tp")
    rows = own.shape[0]
    pair = jnp.concatenate([own[...].astype(f32), other[...].astype(f32)], axis=1)
    block = jnp.where(core == 0, pair, half_turn(pair))
    squares = jnp.sum(block * block, axis=1, keepdims=True)
    high = squares.astype(bf16).astype(f32)
    lane = lax.broadcasted_iota(jnp.int32, (rows, LANES), 1)
    extra = jnp.where(lane == 0, high, jnp.where(lane == 1, squares - high, 0.0))
    scaled = (block * gain[pl.ds(kv, 1), :]).astype(bf16)
    heads = wq.shape[1] // LANES
    step = out.shape[1] * out.shape[2]
    for index, weight in enumerate((wq, wf, wi, wg)):
        part = jnp.dot(scaled, weight[...], preferred_element_type=f32)
        for head in range(heads):
            rows_scr[pl.ds(index * heads + head, rows, stride=step), :] = part[
                :, head * LANES : (head + 1) * LANES
            ]
    for row in range(4 * heads, step):
        rows_scr[pl.ds(row, rows, stride=step), :] = extra
    for row in range(rows):
        piece = rows_scr[pl.ds(row * step, step), :].reshape(out.shape[1:])
        out[SLOTS[row]] = piece.astype(bf16)


def recur_kernel(pieces, state, bound, gain, gated, new_state, width):
    heads = state.shape[0]
    total = jnp.sum(pieces[...].astype(f32), axis=0)
    total = total.reshape(total.shape[0] * total.shape[1], LANES)
    squares = total[4 * heads : 4 * heads + 1, 0:1] + total[4 * heads : 4 * heads + 1, 1:2]
    row_scale = lax.rsqrt(squares / width + epsilon)
    query_pre, forget_pre, value_in, gate_pre = [
        row_scale * total[i * heads : (i + 1) * heads] for i in range(4)
    ]
    forget = bound[...] + (1.0 - bound[...]) * jax.nn.sigmoid(forget_pre)
    forget_down = jnp.transpose(forget)
    query_down = jnp.transpose(jax.nn.silu(query_pre))
    reads = []
    for head in range(heads):
        keep = jnp.broadcast_to(forget_down[:, head : head + 1], state.shape[1:])
        fresh = keep * state[head] + (1.0 - keep) * value_in[head : head + 1]
        new_state[head] = fresh
        reads.append(jnp.sum(query_down[:, head : head + 1] * fresh, axis=0, keepdims=True))
    head_out = jnp.concatenate(reads, axis=0)
    head_out = head_out * lax.rsqrt(
        jnp.mean(head_out * head_out, axis=1, keepdims=True) + epsilon
    )
    value = (head_out * gain[...] * jax.nn.silu(gate_pre)).astype(bf16)
    for peer in range(gated.shape[0]):
        gated[peer] = value


def mix_kernel(own, other, tokens, weight, out, rows_scr, whole_scr):
    core = lax.axis_index("tp")
    rows = tokens.shape[0]
    heads = own.shape[1]
    for row in range(rows):
        rows_scr[0, row * heads : (row + 1) * heads, :] = own[SLOTS[row]].astype(f32)
        rows_scr[1, row * heads : (row + 1) * heads, :] = other[SLOTS[row]].astype(f32)
    for side in range(2):
        source = (core + side) % 2
        for head in range(heads):
            column = (side * heads + head) * LANES
            whole_scr[:, column : column + LANES] = rows_scr[
                source, pl.ds(head, rows, stride=heads), :
            ].astype(bf16)
    added = lax.dot_general(whole_scr[...], weight[...], NT, preferred_element_type=f32)
    mixed = tokens[...].astype(f32) + added
    half = rows // 2
    packed = jnp.concatenate([mixed[:half], mixed[half:]], axis=1)
    packed = jnp.where(core == 0, packed, half_turn(packed)).astype(bf16)
    for peer in range(out.shape[0]):
        out[peer] = packed


def part(index):
    return slice(index * LANES, (index + 1) * LANES)


def split_lanes(low, left, right):
    return jnp.where(low, left, half_turn(right)), jnp.where(low, half_turn(left), right)


def arrange_in_kernel(w_gate, w_up, gain, ins, gains):
    units = w_gate.shape[0]
    low = low_lanes((units, LANES))
    for pair in range(w_gate.shape[1] // (2 * LANES)):
        left, right = part(2 * pair), part(2 * pair + 1)
        for index, weight in enumerate((w_gate, w_up)):
            first, second = split_lanes(low, weight[:, left], weight[:, right])
            ins[0, index * units : (index + 1) * units, part(pair)] = first
            ins[1, index * units : (index + 1) * units, part(pair)] = second
        first, second = split_lanes(
            low[:1], gain[2 * pair : 2 * pair + 1, :], gain[2 * pair + 1 : 2 * pair + 2, :]
        )
        gains[0, pair : pair + 1, :] = first
        gains[1, pair : pair + 1, :] = second


def arrange_out_kernel(w_down, outs):
    low = low_lanes((w_down.shape[0], LANES))
    for pair in range(w_down.shape[1] // (2 * LANES)):
        first, second = split_lanes(low, w_down[:, part(2 * pair)], w_down[:, part(2 * pair + 1)])
        outs[0, :, part(pair)] = first
        outs[1, :, part(pair)] = second


def half_feed(core, chunk, gains, ins, scr):
    blocks, half, _ = chunk.shape
    low = low_lanes((half, LANES))
    squares = jnp.zeros((2 * half, LANES), f32)
    for pair in range(blocks // 2):
        first, second = split_lanes(
            low, chunk[SLOTS[2 * pair]].astype(f32), chunk[SLOTS[2 * pair + 1]].astype(f32)
        )
        value = jnp.concatenate([first, second], axis=0)
        squares = squares + value * value
        scr[:, part(pair)] = (value * gains[core, pair : pair + 1, :]).astype(bf16)
    products = lax.dot_general(scr[...], ins[core], NT, preferred_element_type=f32)
    return products, squares


def own_kernel(chunk, gains, ins, products, squares, scr):
    products[...], squares[...] = half_feed(lax.axis_index("tp"), chunk, gains, ins, scr)


def packed_rows(low, block, turned):
    half = block.shape[0] // 2
    first, second = block[:half], block[half:]
    if turned:
        first, second = second, first
    return split_lanes(low, first, second)


def other_kernel(
    chunk, gains, ins, products, squares, outs, state, theirs, hidden_out, state_hbm, scr, sem
):
    store = pltpu.make_async_copy(state, state_hbm, sem)
    store.start()
    core = lax.axis_index("tp")
    half = chunk.shape[1]
    more, more_squares = half_feed(1 - core, chunk, gains, ins, scr)
    totals = products[...] + jnp.concatenate([more[half:], more[:half]], axis=0)
    both = squares[...] + jnp.concatenate([more_squares[half:], more_squares[:half]], axis=0)
    mean = jnp.sum(both, axis=1, keepdims=True) / (chunk.shape[0] * LANES)
    totals = totals * lax.rsqrt(mean + epsilon)
    units = totals.shape[1] // 2
    hidden = (jax.nn.silu(totals[:, :units]) * totals[:, units:]).astype(bf16)
    hidden_out[...] = hidden
    terms = jnp.dot(hidden, outs[1 - core], preferred_element_type=f32)
    low = low_lanes((half, LANES))
    for pair in range(chunk.shape[0] // 2):
        left, right = packed_rows(low, terms[:, part(pair)], True)
        theirs[SLOTS[2 * pair]] = left.astype(bf16)
        theirs[SLOTS[2 * pair + 1]] = right.astype(bf16)
    store.wait()


def mine_kernel(hidden, outs, mine):
    terms = jnp.dot(hidden[...], outs[lax.axis_index("tp")], preferred_element_type=f32)
    low = low_lanes(mine.shape[1:])
    for pair in range(mine.shape[0] // 2):
        left, right = packed_rows(low, terms[:, part(pair)], False)
        mine[SLOTS[2 * pair]] = left
        mine[SLOTS[2 * pair + 1]] = right


def sum_kernel(mine, theirs, out):
    out[...] = (mine[...] + theirs[...].astype(f32)).astype(bf16)


def finish_kernel(pieces, mixed, out):
    core = lax.axis_index("tp")
    half = mixed.shape[1]
    total = mixed[0].astype(f32) + jnp.sum(pieces[...].astype(f32), axis=0)
    total = jnp.where(core == 0, total, half_turn(total))
    out[:half] = total[:, : LANES // 2].astype(bf16)
    out[half:] = half_turn(total)[:, : LANES // 2].astype(bf16)


def local(
    tokens,
    rec_state,
    norm_gain,
    w_query,
    w_forget,
    w_input,
    w_outgate,
    lower_bound,
    head_gain,
    w_heads_out,
    mixer_gain,
    w_gate,
    w_up,
    w_down,
):
    kv_count = lax.axis_size(KV)
    rows, cols = tokens.shape
    width = norm_gain.shape[0]
    heads = rec_state.shape[1]
    half = rows // 2
    blocks = width // LANES
    shape = pltpu.VMEM
    piece_rows = 4 * heads + 4

    other = lax.ppermute(tokens, "tp", SWAP)
    loads = (
        tokens,
        norm_gain.reshape(blocks, LANES),
        lower_bound.reshape(heads, LANES),
        head_gain.reshape(heads, LANES),
        mixer_gain.reshape(blocks, LANES),
        w_heads_out.T,
    )
    tokens_here, first_gain, bound, gain, second_gain, heads_out = pl.pallas_call(
        load_kernel,
        out_shape=tuple(shape(x.shape, x.dtype) for x in loads),
        in_specs=[IN_HBM] * len(loads),
        out_specs=tuple(in_vmem(len(loads))),
        scratch_shapes=[pltpu.SemaphoreType.DMA((len(loads),))],
        compiler_params=LIMIT,
        cost_estimate=pl.CostEstimate(flops=4000000000, bytes_accessed=20000000, transcendentals=0),
        name="load",
    )(*far(*loads))
    pieces = pl.pallas_call(
        project_kernel,
        out_shape=shape((rows, piece_rows // 4, 4, LANES), bf16),
        in_specs=in_vmem(7),
        out_specs=in_vmem(1)[0],
        scratch_shapes=[pltpu.VMEM((rows * piece_rows, LANES), f32)],
        compiler_params=LIMIT,
        name="project",
    )(
        *held(tokens_here, other, first_gain, w_query, w_forget, w_input, w_outgate)
    )
    pieces = exchanged(pieces)

    gated, new_state = pl.pallas_call(
        lambda *refs: recur_kernel(*refs, width),
        out_shape=(shape((kv_count, heads, LANES), bf16), shape(rec_state.shape[1:], f32)),
        in_specs=in_vmem(4),
        out_specs=tuple(in_vmem(2)),
        compiler_params=LIMIT,
        name="recur",
    )(*held(pieces, rec_state[0], bound, gain))

    own = exchanged(gated)
    other = lax.ppermute(own, "tp", SWAP)
    mixed = pl.pallas_call(
        mix_kernel,
        out_shape=shape((kv_count, half, LANES), bf16),
        in_specs=in_vmem(4),
        out_specs=in_vmem(1)[0],
        scratch_shapes=[
            pltpu.VMEM((2, rows * heads, LANES), f32),
            pltpu.VMEM((rows, 2 * heads * LANES), bf16),
        ],
        compiler_params=LIMIT,
        name="mix",
    )(*held(own, other, tokens_here, heads_out))

    units = w_gate.shape[1]
    ins, gains = pl.pallas_call(
        arrange_in_kernel,
        out_shape=(
            shape((2, 2 * units, width // 2), bf16),
            shape((2, blocks // 2, LANES), f32),
        ),
        in_specs=in_vmem(3),
        out_specs=tuple(in_vmem(2)),
        compiler_params=LIMIT,
        name="arrange_in",
    )(*held(w_gate.T, w_up.T, second_gain))
    outs = pl.pallas_call(
        arrange_out_kernel,
        out_shape=shape((2, units, width // 2), bf16),
        in_specs=in_vmem(1),
        out_specs=in_vmem(1)[0],
        compiler_params=LIMIT,
        name="arrange_out",
    )(*held(w_down))

    own = exchanged(mixed)
    other = lax.ppermute(own, "tp", SWAP)
    chunks = (kv_count, half, LANES)
    products, squares = pl.pallas_call(
        own_kernel,
        out_shape=(shape((rows, 2 * units), f32), shape((rows, LANES), f32)),
        in_specs=in_vmem(3),
        out_specs=tuple(in_vmem(2)),
        scratch_shapes=[pltpu.VMEM((rows, width // 2), bf16)],
        compiler_params=LIMIT,
        name="own",
    )(*held(own, gains, ins))
    theirs, hidden, new_state = pl.pallas_call(
        other_kernel,
        out_shape=(
            shape(chunks, bf16),
            shape((rows, units), bf16),
            pltpu.HBM(new_state.shape, f32),
        ),
        in_specs=in_vmem(7),
        out_specs=tuple(in_vmem(2) + [IN_HBM]),
        scratch_shapes=[pltpu.VMEM((rows, width // 2), bf16), pltpu.SemaphoreType.DMA],
        compiler_params=LIMIT,
        name="other",
    )(*held(other, gains, ins, products, squares, outs, new_state))
    mine = pl.pallas_call(
        mine_kernel,
        out_shape=shape(chunks, f32),
        in_specs=in_vmem(2),
        out_specs=in_vmem(1)[0],
        compiler_params=LIMIT,
        name="mine",
    )(*held(hidden, outs))
    theirs = lax.ppermute(theirs, "tp", SWAP)
    chip_sum = pl.pallas_call(
        sum_kernel,
        out_shape=shape((kv_count, half, LANES), bf16),
        in_specs=in_vmem(2),
        out_specs=in_vmem(1)[0],
        compiler_params=LIMIT,
        name="chip_sum",
    )(*held(mine, theirs))
    down = exchanged(chip_sum)
    result = pl.pallas_call(
        finish_kernel,
        out_shape=jax.ShapeDtypeStruct((rows, cols), bf16),
        in_specs=in_vmem(2),
        out_specs=in_vmem(1)[0],
        compiler_params=LIMIT,
        name="finish",
    )(*held(down, mixed))
    return (result, new_state[None])


def solution(mesh):
    torus = Mesh(
        mesh.devices.reshape(mesh.shape["dp"], 8, 4, mesh.shape["tp"]), ("dp", "kv_0", "kv_1", "tp")
    )
    in_specs = (
        P("dp", KV_TP),
        P(DP_KV, "tp", None, None),
        P(),
        P(KV, "tp"),
        P(KV, "tp"),
        P(KV, "tp"),
        P(KV, "tp"),
        P("tp"),
        P("tp"),
        P(None, KV_TP),
        P(),
        P(None, KV_TP),
        P(None, KV_TP),
        P(KV_TP, None),
    )
    out_specs = (P("dp", KV_TP), P(DP_KV, "tp", None, None))


    return jax.shard_map(local, mesh=torus, in_specs=in_specs, out_specs=out_specs, check_vma=False)
```

```python
import jax
import jax.numpy as jnp
from jax import lax
from jax.experimental import pallas as pl
from jax.experimental.pallas import tpu as pltpu
from jax.sharding import Mesh
from jax.sharding import PartitionSpec as P

LANES = 128
KV = ("kv_0", "kv_1")
KV_TP = ("kv_0", "kv_1", "tp")
DP_KV = ("dp", "kv_0", "kv_1")
SWAP = [(0, 1), (1, 0)]
NT = (((1,), (1,)), ((), ()))

epsilon = 1e-06
bf16, f32 = jnp.bfloat16, jnp.float32


COUNT = 32
OWNERS = [22, 23, 24, 25, 26, 27, 28, 29, 30, 31, 0, 1, 2, 3, 4, 5, 6, 7, 8, 9, 10, 11, 12, 13, 14, 15, 16, 17, 18, 19, 20, 21]
ORDERS = [
    [22, 23, 24, 25, 26, 27, 28, 29, 30, 31, 0, 1, 2, 3, 4, 5, 6, 7, 8, 9, 10, 11, 12, 13, 14, 15, 16, 17, 18, 19, 20, 21],
    [18, 19, 20, 21, 22, 23, 24, 25, 26, 27, 28, 29, 30, 31, 0, 1, 2, 3, 4, 5, 6, 7, 8, 9, 10, 11, 12, 13, 14, 15, 16, 17],
]
LAST_ORDERS = [
    [22, 11, 24, 8, 21, 14, 16, 29, 9, 31, 20, 12, 25, 13, 19, 28, 4, 2, 10, 15, 1, 5, 23, 3, 18, 0, 30, 17, 7, 27, 6, 26],
    [18, 20, 25, 14, 28, 30, 12, 27, 6, 31, 26, 8, 23, 5, 11, 21, 4, 16, 1, 9, 7, 0, 13, 15, 29, 19, 3, 10, 2, 22, 17, 24],
]
FIRST_PLANE = 5
TURNED = [(place // 4 - FIRST_PLANE) % 8 < 4 for place in range(COUNT)]


def teams(orders):
    return [[2 * place + (team ^ TURNED[place]) for place in orders[team]] for team in range(2)]


def exchanged(pieces, axes, groups):
    return lax.all_to_all(
        pieces, axes, split_axis=0, concat_axis=0, axis_index_groups=groups, tiled=True
    )


def my_team():
    plane, core = lax.axis_index("kv_0"), lax.axis_index("tp")
    return jnp.where((plane + 8 - FIRST_PLANE) % 8 < 4, 1 - core, core)


def for_my_team(body):
    mine = my_team()
    for team in range(2):
        pl.when(mine == team)(lambda team=team: body(team))


def low_lanes(shape):
    return lax.broadcasted_iota(jnp.int32, shape, len(shape) - 1) < LANES // 2


def half_turn(x):
    return pltpu.roll(x, LANES // 2, axis=x.ndim - 1)


def in_vmem(count):
    return [pl.BlockSpec(memory_space=pltpu.VMEM)] * count


def held(*arrays):
    return [pltpu.with_memory_space_constraint(array, pltpu.VMEM) for array in arrays]


def far(*arrays):
    return [pltpu.with_memory_space_constraint(array, pltpu.HBM) for array in arrays]


LIMIT = pltpu.CompilerParams(vmem_limit_bytes=8 * 1024 * 1024)
IN_HBM = pl.BlockSpec(memory_space=pltpu.HBM)


def load_kernel(*refs):
    count = len(refs) // 2
    sources, targets, sems = refs[:count], refs[count : 2 * count], refs[-1]
    copies = [
        pltpu.make_async_copy(source, target, sems.at[index])
        for index, (source, target) in enumerate(zip(sources, targets))
    ]
    for copy in copies:
        copy.start()
    for copy in copies:
        copy.wait()


def project_kernel(own, other, gain, wq, wf, wi, wg, out, rows_scr):
    kv, core = lax.axis_index(KV), lax.axis_index("tp")
    rows = own.shape[0]
    pair = jnp.concatenate([own[...].astype(f32), other[...].astype(f32)], axis=1)
    block = jnp.where(core == 0, pair, half_turn(pair))
    squares = jnp.sum(block * block, axis=1, keepdims=True)
    high = squares.astype(bf16).astype(f32)
    lane = lax.broadcasted_iota(jnp.int32, (rows, LANES), 1)
    extra = jnp.where(lane == 0, high, jnp.where(lane == 1, squares - high, 0.0))
    scaled = (block * gain[pl.ds(kv, 1), :]).astype(bf16)
    heads = wq.shape[1] // LANES
    step = out.shape[1] * out.shape[2]
    for index, weight in enumerate((wq, wf, wi, wg)):
        part = jnp.dot(scaled, weight[...], preferred_element_type=f32)
        for head in range(heads):
            rows_scr[pl.ds(index * heads + head, rows, stride=step), :] = part[
                :, head * LANES : (head + 1) * LANES
            ]
    for row in range(4 * heads, step):
        rows_scr[pl.ds(row, rows, stride=step), :] = extra
    for row in range(rows):
        piece = rows_scr[pl.ds(row * step, step), :].reshape(out.shape[1:])
        out[OWNERS.index(row)] = piece.astype(bf16)


def recur_kernel(pieces, state, bound, gain, gated, new_state, width):
    heads = state.shape[0]
    total = jnp.sum(pieces[...].astype(f32), axis=0)
    total = total.reshape(total.shape[0] * total.shape[1], LANES)
    squares = total[4 * heads : 4 * heads + 1, 0:1] + total[4 * heads : 4 * heads + 1, 1:2]
    row_scale = lax.rsqrt(squares / width + epsilon)
    query_pre, forget_pre, value_in, gate_pre = [
        row_scale * total[i * heads : (i + 1) * heads] for i in range(4)
    ]
    forget = bound[...] + (1.0 - bound[...]) * jax.nn.sigmoid(forget_pre)
    forget_down = jnp.transpose(forget)
    query_down = jnp.transpose(jax.nn.silu(query_pre))
    reads = []
    for head in range(heads):
        keep = jnp.broadcast_to(forget_down[:, head : head + 1], state.shape[1:])
        fresh = keep * state[head] + (1.0 - keep) * value_in[head : head + 1]
        new_state[head] = fresh
        reads.append(jnp.sum(query_down[:, head : head + 1] * fresh, axis=0, keepdims=True))
    head_out = jnp.concatenate(reads, axis=0)
    head_out = head_out * lax.rsqrt(
        jnp.mean(head_out * head_out, axis=1, keepdims=True) + epsilon
    )
    value = (head_out * gain[...] * jax.nn.silu(gate_pre)).astype(bf16)
    for peer in range(gated.shape[0]):
        gated[peer] = value


def mix_kernel(own, other, tokens, weight, out, rows_scr, whole_scr):
    def body(team):
        rows = tokens.shape[0]
        heads = own.shape[1]
        for row in range(rows):
            place = slice(row * heads, (row + 1) * heads)
            side = 1 - team if TURNED[row] else team
            rows_scr[side, place, :] = own[ORDERS[team].index(row)].astype(f32)
            rows_scr[1 - side, place, :] = other[ORDERS[1 - team].index(row)].astype(f32)
        for side in range(2):
            for head in range(heads):
                column = (side * heads + head) * LANES
                whole_scr[:, column : column + LANES] = rows_scr[
                    side, pl.ds(head, rows, stride=heads), :
                ].astype(bf16)
        added = lax.dot_general(whole_scr[...], weight[...], NT, preferred_element_type=f32)
        mixed = tokens[...].astype(f32) + added
        half = rows // 2
        packed = jnp.concatenate([mixed[:half], mixed[half:]], axis=1)
        packed = (half_turn(packed) if team else packed).astype(bf16)
        for peer in range(out.shape[0]):
            out[peer] = packed

    for_my_team(body)


def part(index):
    return slice(index * LANES, (index + 1) * LANES)


def split_lanes(low, left, right):
    return jnp.where(low, left, half_turn(right)), jnp.where(low, half_turn(left), right)


def by_team(pair, halves):
    return halves[::-1] if TURNED[2 * pair] else halves


def arrange_in_kernel(w_gate, w_up, gain, ins, gains):
    units = w_gate.shape[0]
    low = low_lanes((units, LANES))
    for pair in range(w_gate.shape[1] // (2 * LANES)):
        left, right = part(2 * pair), part(2 * pair + 1)
        for index, weight in enumerate((w_gate, w_up)):
            first, second = by_team(pair, split_lanes(low, weight[:, left], weight[:, right]))
            ins[0, index * units : (index + 1) * units, part(pair)] = first
            ins[1, index * units : (index + 1) * units, part(pair)] = second
        first, second = by_team(
            pair,
            split_lanes(
                low[:1], gain[2 * pair : 2 * pair + 1, :], gain[2 * pair + 1 : 2 * pair + 2, :]
            ),
        )
        gains[0, pair : pair + 1, :] = first
        gains[1, pair : pair + 1, :] = second


def arrange_out_kernel(w_down, outs):
    low = low_lanes((w_down.shape[0], LANES))
    for pair in range(w_down.shape[1] // (2 * LANES)):
        first, second = by_team(
            pair, split_lanes(low, w_down[:, part(2 * pair)], w_down[:, part(2 * pair + 1)])
        )
        outs[0, :, part(pair)] = first
        outs[1, :, part(pair)] = second


def half_feed(team, chunk, gains, ins, scr):
    blocks, half, _ = chunk.shape
    low = low_lanes((half, LANES))
    squares = jnp.zeros((2 * half, LANES), f32)
    for pair in range(blocks // 2):
        first, second = split_lanes(
            low,
            chunk[ORDERS[team].index(2 * pair)].astype(f32),
            chunk[ORDERS[team].index(2 * pair + 1)].astype(f32),
        )
        value = jnp.concatenate([first, second], axis=0)
        squares = squares + value * value
        scr[:, part(pair)] = (value * gains[team, pair : pair + 1, :]).astype(bf16)
    products = lax.dot_general(scr[...], ins[team], NT, preferred_element_type=f32)
    return products, squares


def own_kernel(chunk, gains, ins, products, squares, scr):
    def body(team):
        products[...], squares[...] = half_feed(team, chunk, gains, ins, scr)

    for_my_team(body)


def packed_rows(low, block, turned):
    half = block.shape[0] // 2
    first, second = block[:half], block[half:]
    if turned:
        first, second = second, first
    return split_lanes(low, first, second)


def other_kernel(
    chunk, gains, ins, products, squares, outs, state, theirs, hidden_out, state_hbm, scr, sem
):
    store = pltpu.make_async_copy(state, state_hbm, sem)
    store.start()

    def body(team):
        half = chunk.shape[1]
        more, more_squares = half_feed(1 - team, chunk, gains, ins, scr)
        totals = products[...] + jnp.concatenate([more[half:], more[:half]], axis=0)
        both = squares[...] + jnp.concatenate([more_squares[half:], more_squares[:half]], axis=0)
        mean = jnp.sum(both, axis=1, keepdims=True) / (chunk.shape[0] * LANES)
        totals = totals * lax.rsqrt(mean + epsilon)
        units = totals.shape[1] // 2
        hidden = (jax.nn.silu(totals[:, :units]) * totals[:, units:]).astype(bf16)
        hidden_out[...] = hidden
        terms = jnp.dot(hidden, outs[1 - team], preferred_element_type=f32)
        low = low_lanes((half, LANES))
        for pair in range(chunk.shape[0] // 2):
            left, right = packed_rows(low, terms[:, part(pair)], True)
            theirs[LAST_ORDERS[1 - team].index(2 * pair)] = left.astype(bf16)
            theirs[LAST_ORDERS[1 - team].index(2 * pair + 1)] = right.astype(bf16)

    for_my_team(body)
    store.wait()


def mine_kernel(hidden, outs, mine):
    def body(team):
        terms = jnp.dot(hidden[...], outs[team], preferred_element_type=f32)
        low = low_lanes(mine.shape[1:])
        for pair in range(mine.shape[0] // 2):
            left, right = packed_rows(low, terms[:, part(pair)], False)
            mine[LAST_ORDERS[team].index(2 * pair)] = left
            mine[LAST_ORDERS[team].index(2 * pair + 1)] = right

    for_my_team(body)


def sum_kernel(mine, theirs, out):
    out[...] = (mine[...] + theirs[...].astype(f32)).astype(bf16)


def finish_kernel(pieces, mixed, out):
    half = mixed.shape[1]
    total = mixed[0].astype(f32) + jnp.sum(pieces[...].astype(f32), axis=0)
    total = jnp.where(my_team() == 0, total, half_turn(total))
    out[:half] = total[:, : LANES // 2].astype(bf16)
    out[half:] = half_turn(total)[:, : LANES // 2].astype(bf16)


def local(
    tokens,
    rec_state,
    norm_gain,
    w_query,
    w_forget,
    w_input,
    w_outgate,
    lower_bound,
    head_gain,
    w_heads_out,
    mixer_gain,
    w_gate,
    w_up,
    w_down,
):
    kv_count = lax.axis_size(KV)
    rows, cols = tokens.shape
    width = norm_gain.shape[0]
    heads = rec_state.shape[1]
    half = rows // 2
    blocks = width // LANES
    shape = pltpu.VMEM
    piece_rows = 4 * heads + 4

    other = lax.ppermute(tokens, "tp", SWAP)
    loads = (
        tokens,
        norm_gain.reshape(blocks, LANES),
        lower_bound.reshape(heads, LANES),
        head_gain.reshape(heads, LANES),
        mixer_gain.reshape(blocks, LANES),
        w_heads_out.T,
    )
    tokens_here, first_gain, bound, gain, second_gain, heads_out = pl.pallas_call(
        load_kernel,
        out_shape=tuple(shape(x.shape, x.dtype) for x in loads),
        in_specs=[IN_HBM] * len(loads),
        out_specs=tuple(in_vmem(len(loads))),
        scratch_shapes=[pltpu.SemaphoreType.DMA((len(loads),))],
        compiler_params=LIMIT,
        cost_estimate=pl.CostEstimate(flops=4000000000, bytes_accessed=20000000, transcendentals=0),
        name="load",
    )(*far(*loads))
    pieces = pl.pallas_call(
        project_kernel,
        out_shape=shape((rows, piece_rows // 4, 4, LANES), bf16),
        in_specs=in_vmem(7),
        out_specs=in_vmem(1)[0],
        scratch_shapes=[pltpu.VMEM((rows * piece_rows, LANES), f32)],
        compiler_params=LIMIT,
        name="project",
    )(
        *held(tokens_here, other, first_gain, w_query, w_forget, w_input, w_outgate)
    )
    pieces = exchanged(pieces, KV, [OWNERS])

    gated, new_state = pl.pallas_call(
        lambda *refs: recur_kernel(*refs, width),
        out_shape=(shape((kv_count, heads, LANES), bf16), shape(rec_state.shape[1:], f32)),
        in_specs=in_vmem(4),
        out_specs=tuple(in_vmem(2)),
        compiler_params=LIMIT,
        name="recur",
    )(*held(pieces, rec_state[0], bound, gain))

    own = exchanged(gated, KV_TP, teams(ORDERS))
    other = lax.ppermute(own, "tp", SWAP)
    mixed = pl.pallas_call(
        mix_kernel,
        out_shape=shape((kv_count, half, LANES), bf16),
        in_specs=in_vmem(4),
        out_specs=in_vmem(1)[0],
        scratch_shapes=[
            pltpu.VMEM((2, rows * heads, LANES), f32),
            pltpu.VMEM((rows, 2 * heads * LANES), bf16),
        ],
        compiler_params=LIMIT,
        name="mix",
    )(*held(own, other, tokens_here, heads_out))

    units = w_gate.shape[1]
    ins, gains = pl.pallas_call(
        arrange_in_kernel,
        out_shape=(
            shape((2, 2 * units, width // 2), bf16),
            shape((2, blocks // 2, LANES), f32),
        ),
        in_specs=in_vmem(3),
        out_specs=tuple(in_vmem(2)),
        compiler_params=LIMIT,
        name="arrange_in",
    )(*held(w_gate.T, w_up.T, second_gain))
    outs = pl.pallas_call(
        arrange_out_kernel,
        out_shape=shape((2, units, width // 2), bf16),
        in_specs=in_vmem(1),
        out_specs=in_vmem(1)[0],
        compiler_params=LIMIT,
        name="arrange_out",
    )(*held(w_down))

    own = exchanged(mixed, KV_TP, teams(ORDERS))
    other = lax.ppermute(own, "tp", SWAP)
    chunks = (kv_count, half, LANES)
    products, squares = pl.pallas_call(
        own_kernel,
        out_shape=(shape((rows, 2 * units), f32), shape((rows, LANES), f32)),
        in_specs=in_vmem(3),
        out_specs=tuple(in_vmem(2)),
        scratch_shapes=[pltpu.VMEM((rows, width // 2), bf16)],
        compiler_params=LIMIT,
        name="own",
    )(*held(own, gains, ins))
    theirs, hidden, new_state = pl.pallas_call(
        other_kernel,
        out_shape=(
            shape(chunks, bf16),
            shape((rows, units), bf16),
            pltpu.HBM(new_state.shape, f32),
        ),
        in_specs=in_vmem(7),
        out_specs=tuple(in_vmem(2) + [IN_HBM]),
        scratch_shapes=[pltpu.VMEM((rows, width // 2), bf16), pltpu.SemaphoreType.DMA],
        compiler_params=LIMIT,
        name="other",
    )(*held(other, gains, ins, products, squares, outs, new_state))
    mine = pl.pallas_call(
        mine_kernel,
        out_shape=shape(chunks, f32),
        in_specs=in_vmem(2),
        out_specs=in_vmem(1)[0],
        compiler_params=LIMIT,
        name="mine",
    )(*held(hidden, outs))
    theirs = lax.ppermute(theirs, "tp", SWAP)
    chip_sum = pl.pallas_call(
        sum_kernel,
        out_shape=shape((kv_count, half, LANES), bf16),
        in_specs=in_vmem(2),
        out_specs=in_vmem(1)[0],
        compiler_params=LIMIT,
        name="chip_sum",
    )(*held(mine, theirs))
    down = exchanged(chip_sum, KV_TP, teams(LAST_ORDERS))
    result = pl.pallas_call(
        finish_kernel,
        out_shape=jax.ShapeDtypeStruct((rows, cols), bf16),
        in_specs=in_vmem(2),
        out_specs=in_vmem(1)[0],
        compiler_params=LIMIT,
        name="finish",
    )(*held(down, mixed))
    return (result, new_state[None])


def solution(mesh):
    torus = Mesh(
        mesh.devices.reshape(mesh.shape["dp"], 8, 4, mesh.shape["tp"]), ("dp", "kv_0", "kv_1", "tp")
    )
    in_specs = (
        P("dp", KV_TP),
        P(DP_KV, "tp", None, None),
        P(),
        P(KV, "tp"),
        P(KV, "tp"),
        P(KV, "tp"),
        P(KV, "tp"),
        P("tp"),
        P("tp"),
        P(None, KV_TP),
        P(),
        P(None, KV_TP),
        P(None, KV_TP),
        P(KV_TP, None),
    )
    out_specs = (P("dp", KV_TP), P(DP_KV, "tp", None, None))


    return jax.shard_map(local, mesh=torus, in_specs=in_specs, out_specs=out_specs, check_vma=False)
```

```python
import jax
import jax.numpy as jnp
from jax import lax
from jax.experimental import pallas as pl
from jax.experimental.pallas import tpu as pltpu
from jax.sharding import Mesh
from jax.sharding import PartitionSpec as P

LANES = 128
KV = ("kv_0", "kv_1")
KV_TP = ("kv_0", "kv_1", "tp")
DP_KV = ("dp", "kv_0", "kv_1")
SWAP = [(0, 1), (1, 0)]
NT = (((1,), (1,)), ((), ()))

epsilon = 1e-06
bf16, f32 = jnp.bfloat16, jnp.float32


COUNT = 32
OWNERS = [22, 23, 24, 25, 26, 27, 28, 29, 30, 31, 0, 1, 2, 3, 4, 5, 6, 7, 8, 9, 10, 11, 12, 13, 14, 15, 16, 17, 18, 19, 20, 21]
ORDERS = [
    [22, 23, 24, 25, 26, 27, 28, 29, 30, 31, 0, 1, 2, 3, 4, 5, 6, 7, 8, 9, 10, 11, 12, 13, 14, 15, 16, 17, 18, 19, 20, 21],
    [18, 19, 20, 21, 22, 23, 24, 25, 26, 27, 28, 29, 30, 31, 0, 1, 2, 3, 4, 5, 6, 7, 8, 9, 10, 11, 12, 13, 14, 15, 16, 17],
]
LAST_ORDERS = [
    [22, 8, 2, 14, 7, 1, 5, 21, 20, 6, 0, 31, 9, 11, 28, 16, 29, 17, 15, 27, 13, 3, 26, 4, 30, 10, 23, 24, 12, 25, 18, 19],
    [18, 29, 20, 16, 28, 12, 25, 21, 7, 2, 8, 15, 24, 9, 22, 31, 19, 1, 14, 6, 27, 17, 0, 10, 5, 26, 4, 13, 30, 23, 11, 3],
]
FIRST_PLANE = 5
TURNED = [(place // 4 - FIRST_PLANE) % 8 < 4 for place in range(COUNT)]


def teams(orders):
    return [[2 * place + (team ^ TURNED[place]) for place in orders[team]] for team in range(2)]


def exchanged(pieces, axes, groups):
    return lax.all_to_all(
        pieces, axes, split_axis=0, concat_axis=0, axis_index_groups=groups, tiled=True
    )


def my_team():
    plane, core = lax.axis_index("kv_0"), lax.axis_index("tp")
    return jnp.where((plane + 8 - FIRST_PLANE) % 8 < 4, 1 - core, core)


def for_my_team(body):
    mine = my_team()
    for team in range(2):
        pl.when(mine == team)(lambda team=team: body(team))


def low_lanes(shape):
    return lax.broadcasted_iota(jnp.int32, shape, len(shape) - 1) < LANES // 2


def half_turn(x):
    return pltpu.roll(x, LANES // 2, axis=x.ndim - 1)


def in_vmem(count):
    return [pl.BlockSpec(memory_space=pltpu.VMEM)] * count


def held(*arrays):
    return [pltpu.with_memory_space_constraint(array, pltpu.VMEM) for array in arrays]


def far(*arrays):
    return [pltpu.with_memory_space_constraint(array, pltpu.HBM) for array in arrays]


LIMIT = pltpu.CompilerParams(vmem_limit_bytes=8 * 1024 * 1024)
IN_HBM = pl.BlockSpec(memory_space=pltpu.HBM)


def load_kernel(*refs):
    count = len(refs) // 2
    sources, targets, sems = refs[:count], refs[count : 2 * count], refs[-1]
    copies = [
        pltpu.make_async_copy(source, target, sems.at[index])
        for index, (source, target) in enumerate(zip(sources, targets))
    ]
    for copy in copies:
        copy.start()
    for copy in copies:
        copy.wait()


def project_kernel(own, other, gain, wq, wf, wi, wg, out, rows_scr):
    kv, core = lax.axis_index(KV), lax.axis_index("tp")
    rows = own.shape[0]
    pair = jnp.concatenate([own[...].astype(f32), other[...].astype(f32)], axis=1)
    block = jnp.where(core == 0, pair, half_turn(pair))
    squares = jnp.sum(block * block, axis=1, keepdims=True)
    high = squares.astype(bf16).astype(f32)
    lane = lax.broadcasted_iota(jnp.int32, (rows, LANES), 1)
    extra = jnp.where(lane == 0, high, jnp.where(lane == 1, squares - high, 0.0))
    scaled = (block * gain[pl.ds(kv, 1), :]).astype(bf16)
    heads = wq.shape[1] // LANES
    step = out.shape[1] * out.shape[2]
    for index, weight in enumerate((wq, wf, wi, wg)):
        part = jnp.dot(scaled, weight[...], preferred_element_type=f32)
        for head in range(heads):
            rows_scr[pl.ds(index * heads + head, rows, stride=step), :] = part[
                :, head * LANES : (head + 1) * LANES
            ]
    for row in range(4 * heads, step):
        rows_scr[pl.ds(row, rows, stride=step), :] = extra
    for row in range(rows):
        piece = rows_scr[pl.ds(row * step, step), :].reshape(out.shape[1:])
        out[OWNERS.index(row)] = piece.astype(bf16)


def recur_kernel(pieces, state, bound, gain, gated, new_state, width):
    heads = state.shape[0]
    total = jnp.sum(pieces[...].astype(f32), axis=0)
    total = total.reshape(total.shape[0] * total.shape[1], LANES)
    squares = total[4 * heads : 4 * heads + 1, 0:1] + total[4 * heads : 4 * heads + 1, 1:2]
    row_scale = lax.rsqrt(squares / width + epsilon)
    query_pre, forget_pre, value_in, gate_pre = [
        row_scale * total[i * heads : (i + 1) * heads] for i in range(4)
    ]
    forget = bound[...] + (1.0 - bound[...]) * jax.nn.sigmoid(forget_pre)
    forget_down = jnp.transpose(forget)
    query_down = jnp.transpose(jax.nn.silu(query_pre))
    reads = []
    for head in range(heads):
        keep = jnp.broadcast_to(forget_down[:, head : head + 1], state.shape[1:])
        fresh = keep * state[head] + (1.0 - keep) * value_in[head : head + 1]
        new_state[head] = fresh
        reads.append(jnp.sum(query_down[:, head : head + 1] * fresh, axis=0, keepdims=True))
    head_out = jnp.concatenate(reads, axis=0)
    head_out = head_out * lax.rsqrt(
        jnp.mean(head_out * head_out, axis=1, keepdims=True) + epsilon
    )
    value = (head_out * gain[...] * jax.nn.silu(gate_pre)).astype(bf16)
    for peer in range(gated.shape[0]):
        gated[peer] = value


def mix_kernel(own, other, tokens, weight, out, rows_scr, whole_scr):
    def body(team):
        rows = tokens.shape[0]
        heads = own.shape[1]
        for row in range(rows):
            place = slice(row * heads, (row + 1) * heads)
            side = 1 - team if TURNED[row] else team
            rows_scr[side, place, :] = own[ORDERS[team].index(row)].astype(f32)
            rows_scr[1 - side, place, :] = other[ORDERS[1 - team].index(row)].astype(f32)
        for side in range(2):
            for head in range(heads):
                column = (side * heads + head) * LANES
                whole_scr[:, column : column + LANES] = rows_scr[
                    side, pl.ds(head, rows, stride=heads), :
                ].astype(bf16)
        added = lax.dot_general(whole_scr[...], weight[...], NT, preferred_element_type=f32)
        mixed = tokens[...].astype(f32) + added
        half = rows // 2
        packed = jnp.concatenate([mixed[:half], mixed[half:]], axis=1)
        packed = (half_turn(packed) if team else packed).astype(bf16)
        for peer in range(out.shape[0]):
            out[peer] = packed

    for_my_team(body)


def part(index):
    return slice(index * LANES, (index + 1) * LANES)


def split_lanes(low, left, right):
    return jnp.where(low, left, half_turn(right)), jnp.where(low, half_turn(left), right)


def by_team(pair, halves):
    return halves[::-1] if TURNED[2 * pair] else halves


def arrange_in_kernel(w_gate, w_up, gain, ins, gains):
    units = w_gate.shape[0]
    low = low_lanes((units, LANES))
    for pair in range(w_gate.shape[1] // (2 * LANES)):
        left, right = part(2 * pair), part(2 * pair + 1)
        for index, weight in enumerate((w_gate, w_up)):
            first, second = by_team(pair, split_lanes(low, weight[:, left], weight[:, right]))
            ins[0, index * units : (index + 1) * units, part(pair)] = first
            ins[1, index * units : (index + 1) * units, part(pair)] = second
        first, second = by_team(
            pair,
            split_lanes(
                low[:1], gain[2 * pair : 2 * pair + 1, :], gain[2 * pair + 1 : 2 * pair + 2, :]
            ),
        )
        gains[0, pair : pair + 1, :] = first
        gains[1, pair : pair + 1, :] = second


def half_feed(team, chunk, gains, ins, scr):
    blocks, half, _ = chunk.shape
    low = low_lanes((half, LANES))
    squares = jnp.zeros((2 * half, LANES), f32)
    for pair in range(blocks // 2):
        first, second = split_lanes(
            low,
            chunk[ORDERS[team].index(2 * pair)].astype(f32),
            chunk[ORDERS[team].index(2 * pair + 1)].astype(f32),
        )
        value = jnp.concatenate([first, second], axis=0)
        squares = squares + value * value
        scr[:, part(pair)] = (value * gains[team, pair : pair + 1, :]).astype(bf16)
    products = lax.dot_general(scr[...], ins[team], NT, preferred_element_type=f32)
    return products, squares


def own_kernel(
    chunk, gains, ins, w_down, state, products, squares, outs, state_hbm, scr, sem
):
    store = pltpu.make_async_copy(state, state_hbm, sem)
    store.start()

    def body(team):
        products[...], squares[...] = half_feed(team, chunk, gains, ins, scr)

    for_my_team(body)
    low = low_lanes((w_down.shape[0], LANES))
    for pair in range(w_down.shape[1] // (2 * LANES)):
        first, second = by_team(
            pair, split_lanes(low, w_down[:, part(2 * pair)], w_down[:, part(2 * pair + 1)])
        )
        outs[0, :, part(pair)] = first
        outs[1, :, part(pair)] = second
    store.wait()


def packed_rows(low, block, turned):
    half = block.shape[0] // 2
    first, second = block[:half], block[half:]
    if turned:
        first, second = second, first
    return split_lanes(low, first, second)


def other_kernel(chunk, gains, ins, products, squares, outs, theirs, hidden_out, scr):
    def body(team):
        half = chunk.shape[1]
        more, more_squares = half_feed(1 - team, chunk, gains, ins, scr)
        totals = products[...] + jnp.concatenate([more[half:], more[:half]], axis=0)
        both = squares[...] + jnp.concatenate([more_squares[half:], more_squares[:half]], axis=0)
        mean = jnp.sum(both, axis=1, keepdims=True) / (chunk.shape[0] * LANES)
        totals = totals * lax.rsqrt(mean + epsilon)
        units = totals.shape[1] // 2
        hidden = (jax.nn.silu(totals[:, :units]) * totals[:, units:]).astype(bf16)
        hidden_out[...] = hidden
        terms = jnp.dot(hidden, outs[1 - team], preferred_element_type=f32)
        low = low_lanes((half, LANES))
        for pair in range(chunk.shape[0] // 2):
            left, right = packed_rows(low, terms[:, part(pair)], True)
            theirs[LAST_ORDERS[1 - team].index(2 * pair)] = left.astype(bf16)
            theirs[LAST_ORDERS[1 - team].index(2 * pair + 1)] = right.astype(bf16)

    for_my_team(body)


def mine_kernel(hidden, outs, mine):
    def body(team):
        terms = jnp.dot(hidden[...], outs[team], preferred_element_type=f32)
        low = low_lanes(mine.shape[1:])
        for pair in range(mine.shape[0] // 2):
            left, right = packed_rows(low, terms[:, part(pair)], False)
            mine[LAST_ORDERS[team].index(2 * pair)] = left
            mine[LAST_ORDERS[team].index(2 * pair + 1)] = right

    for_my_team(body)


def sum_kernel(mine, theirs, out):
    out[...] = (mine[...] + theirs[...].astype(f32)).astype(bf16)


def finish_kernel(pieces, mixed, out):
    half = mixed.shape[1]
    total = mixed[0].astype(f32) + jnp.sum(pieces[...].astype(f32), axis=0)
    total = jnp.where(my_team() == 0, total, half_turn(total))
    out[:half] = total[:, : LANES // 2].astype(bf16)
    out[half:] = half_turn(total)[:, : LANES // 2].astype(bf16)


def local(
    tokens,
    rec_state,
    norm_gain,
    w_query,
    w_forget,
    w_input,
    w_outgate,
    lower_bound,
    head_gain,
    w_heads_out,
    mixer_gain,
    w_gate,
    w_up,
    w_down,
):
    kv_count = lax.axis_size(KV)
    rows, cols = tokens.shape
    width = norm_gain.shape[0]
    heads = rec_state.shape[1]
    half = rows // 2
    blocks = width // LANES
    shape = pltpu.VMEM
    piece_rows = 4 * heads + 4

    other = lax.ppermute(tokens, "tp", SWAP)
    loads = (
        tokens,
        norm_gain.reshape(blocks, LANES),
        lower_bound.reshape(heads, LANES),
        head_gain.reshape(heads, LANES),
        mixer_gain.reshape(blocks, LANES),
        w_heads_out.T,
    )
    tokens_here, first_gain, bound, gain, second_gain, heads_out = pl.pallas_call(
        load_kernel,
        out_shape=tuple(shape(x.shape, x.dtype) for x in loads),
        in_specs=[IN_HBM] * len(loads),
        out_specs=tuple(in_vmem(len(loads))),
        scratch_shapes=[pltpu.SemaphoreType.DMA((len(loads),))],
        compiler_params=LIMIT,
        cost_estimate=pl.CostEstimate(flops=4000000000, bytes_accessed=20000000, transcendentals=0),
        name="load",
    )(*far(*loads))
    pieces = pl.pallas_call(
        project_kernel,
        out_shape=shape((rows, piece_rows // 4, 4, LANES), bf16),
        in_specs=in_vmem(7),
        out_specs=in_vmem(1)[0],
        scratch_shapes=[pltpu.VMEM((rows * piece_rows, LANES), f32)],
        compiler_params=LIMIT,
        name="project",
    )(
        *held(tokens_here, other, first_gain, w_query, w_forget, w_input, w_outgate)
    )
    pieces = exchanged(pieces, KV, [OWNERS])

    gated, new_state = pl.pallas_call(
        lambda *refs: recur_kernel(*refs, width),
        out_shape=(shape((kv_count, heads, LANES), bf16), shape(rec_state.shape[1:], f32)),
        in_specs=in_vmem(4),
        out_specs=tuple(in_vmem(2)),
        compiler_params=LIMIT,
        name="recur",
    )(*held(pieces, rec_state[0], bound, gain))

    own = exchanged(gated, KV_TP, teams(ORDERS))
    other = lax.ppermute(own, "tp", SWAP)
    mixed = pl.pallas_call(
        mix_kernel,
        out_shape=shape((kv_count, half, LANES), bf16),
        in_specs=in_vmem(4),
        out_specs=in_vmem(1)[0],
        scratch_shapes=[
            pltpu.VMEM((2, rows * heads, LANES), f32),
            pltpu.VMEM((rows, 2 * heads * LANES), bf16),
        ],
        compiler_params=LIMIT,
        name="mix",
    )(*held(own, other, tokens_here, heads_out))

    units = w_gate.shape[1]
    ins, gains = pl.pallas_call(
        arrange_in_kernel,
        out_shape=(
            shape((2, 2 * units, width // 2), bf16),
            shape((2, blocks // 2, LANES), f32),
        ),
        in_specs=in_vmem(3),
        out_specs=tuple(in_vmem(2)),
        compiler_params=LIMIT,
        name="arrange_in",
    )(*held(w_gate.T, w_up.T, second_gain))

    own = exchanged(mixed, KV_TP, teams(ORDERS))
    other = lax.ppermute(own, "tp", SWAP)
    chunks = (kv_count, half, LANES)
    products, squares, outs, new_state = pl.pallas_call(
        own_kernel,
        out_shape=(
            shape((rows, 2 * units), f32),
            shape((rows, LANES), f32),
            shape((2, units, width // 2), bf16),
            pltpu.HBM(new_state.shape, f32),
        ),
        in_specs=in_vmem(5),
        out_specs=tuple(in_vmem(3) + [IN_HBM]),
        scratch_shapes=[pltpu.VMEM((rows, width // 2), bf16), pltpu.SemaphoreType.DMA],
        compiler_params=LIMIT,
        name="own",
    )(*held(own, gains, ins, w_down, new_state))
    theirs, hidden = pl.pallas_call(
        other_kernel,
        out_shape=(shape(chunks, bf16), shape((rows, units), bf16)),
        in_specs=in_vmem(6),
        out_specs=tuple(in_vmem(2)),
        scratch_shapes=[pltpu.VMEM((rows, width // 2), bf16)],
        compiler_params=LIMIT,
        name="other",
    )(*held(other, gains, ins, products, squares, outs))
    mine = pl.pallas_call(
        mine_kernel,
        out_shape=shape(chunks, f32),
        in_specs=in_vmem(2),
        out_specs=in_vmem(1)[0],
        compiler_params=LIMIT,
        name="mine",
    )(*held(hidden, outs))
    theirs = lax.ppermute(theirs, "tp", SWAP)
    chip_sum = pl.pallas_call(
        sum_kernel,
        out_shape=shape((kv_count, half, LANES), bf16),
        in_specs=in_vmem(2),
        out_specs=in_vmem(1)[0],
        compiler_params=LIMIT,
        name="chip_sum",
    )(*held(mine, theirs))
    down = exchanged(chip_sum, KV_TP, teams(LAST_ORDERS))
    result = pl.pallas_call(
        finish_kernel,
        out_shape=jax.ShapeDtypeStruct((rows, cols), bf16),
        in_specs=in_vmem(2),
        out_specs=in_vmem(1)[0],
        compiler_params=LIMIT,
        name="finish",
    )(*held(down, mixed))
    return (result, new_state[None])


def solution(mesh):
    torus = Mesh(
        mesh.devices.reshape(mesh.shape["dp"], 8, 4, mesh.shape["tp"]), ("dp", "kv_0", "kv_1", "tp")
    )
    in_specs = (
        P("dp", KV_TP),
        P(DP_KV, "tp", None, None),
        P(),
        P(KV, "tp"),
        P(KV, "tp"),
        P(KV, "tp"),
        P(KV, "tp"),
        P("tp"),
        P("tp"),
        P(None, KV_TP),
        P(),
        P(None, KV_TP),
        P(None, KV_TP),
        P(KV_TP, None),
    )
    out_specs = (P("dp", KV_TP), P(DP_KV, "tp", None, None))


    return jax.shard_map(local, mesh=torus, in_specs=in_specs, out_specs=out_specs, check_vma=False)
```

```python
import jax
import jax.numpy as jnp
from jax import lax
from jax.experimental import pallas as pl
from jax.experimental.pallas import tpu as pltpu
from jax.sharding import Mesh
from jax.sharding import PartitionSpec as P

LANES = 128
KV = ("kv_0", "kv_1")
KV_TP = ("kv_0", "kv_1", "tp")
DP_KV = ("dp", "kv_0", "kv_1")
SWAP = [(0, 1), (1, 0)]
NT = (((1,), (1,)), ((), ()))

epsilon = 1e-06
bf16, f32 = jnp.bfloat16, jnp.float32


COUNT = 32
OWNERS = [22, 23, 24, 25, 26, 27, 28, 29, 30, 31, 0, 1, 2, 3, 4, 5, 6, 7, 8, 9, 10, 11, 12, 13, 14, 15, 16, 17, 18, 19, 20, 21]
ORDERS = [
    [22, 23, 24, 25, 26, 27, 28, 29, 30, 31, 0, 1, 2, 3, 4, 5, 6, 7, 8, 9, 10, 11, 12, 13, 14, 15, 16, 17, 18, 19, 20, 21],
    [18, 19, 20, 21, 22, 23, 24, 25, 26, 27, 28, 29, 30, 31, 0, 1, 2, 3, 4, 5, 6, 7, 8, 9, 10, 11, 12, 13, 14, 15, 16, 17],
]
LAST_ORDERS = [
    [22, 8, 2, 14, 7, 1, 5, 21, 20, 6, 0, 31, 9, 11, 28, 16, 29, 17, 15, 27, 13, 3, 26, 4, 30, 10, 23, 24, 12, 25, 18, 19],
    [18, 29, 20, 16, 28, 12, 25, 21, 7, 2, 8, 15, 24, 9, 22, 31, 19, 1, 14, 6, 27, 17, 0, 10, 5, 26, 4, 13, 30, 23, 11, 3],
]
FIRST_PLANE = 5
TURNED = [(place // 4 - FIRST_PLANE) % 8 < 4 for place in range(COUNT)]


def teams(orders):
    return [[2 * place + (team ^ TURNED[place]) for place in orders[team]] for team in range(2)]


def exchanged(pieces, axes, groups):
    return lax.all_to_all(
        pieces, axes, split_axis=0, concat_axis=0, axis_index_groups=groups, tiled=True
    )


def my_team():
    plane, core = lax.axis_index("kv_0"), lax.axis_index("tp")
    return jnp.where((plane + 8 - FIRST_PLANE) % 8 < 4, 1 - core, core)


def for_my_team(body):
    mine = my_team()
    for team in range(2):
        pl.when(mine == team)(lambda team=team: body(team))


def low_lanes(shape):
    return lax.broadcasted_iota(jnp.int32, shape, len(shape) - 1) < LANES // 2


def half_turn(x):
    return pltpu.roll(x, LANES // 2, axis=x.ndim - 1)


def in_vmem(count):
    return [pl.BlockSpec(memory_space=pltpu.VMEM)] * count


def held(*arrays):
    return [pltpu.with_memory_space_constraint(array, pltpu.VMEM) for array in arrays]


def far(*arrays):
    return [pltpu.with_memory_space_constraint(array, pltpu.HBM) for array in arrays]


LIMIT = pltpu.CompilerParams(vmem_limit_bytes=8 * 1024 * 1024)
IN_HBM = pl.BlockSpec(memory_space=pltpu.HBM)


def load_kernel(*refs):
    count = len(refs) // 2
    sources, targets, sems = refs[:count], refs[count : 2 * count], refs[-1]
    copies = [
        pltpu.make_async_copy(source, target, sems.at[index])
        for index, (source, target) in enumerate(zip(sources, targets))
    ]
    for copy in copies:
        copy.start()
    for copy in copies:
        copy.wait()


def project_kernel(own, other, gain, wq, wf, wi, wg, out, rows_scr):
    kv, core = lax.axis_index(KV), lax.axis_index("tp")
    rows = own.shape[0]
    pair = jnp.concatenate([own[...].astype(f32), other[...].astype(f32)], axis=1)
    block = jnp.where(core == 0, pair, half_turn(pair))
    squares = jnp.sum(block * block, axis=1, keepdims=True)
    high = squares.astype(bf16).astype(f32)
    lane = lax.broadcasted_iota(jnp.int32, (rows, LANES), 1)
    extra = jnp.where(lane == 0, high, jnp.where(lane == 1, squares - high, 0.0))
    scaled = (block * gain[pl.ds(kv, 1), :]).astype(bf16)
    heads = wq.shape[1] // LANES
    step = out.shape[1] * out.shape[2]
    for index, weight in enumerate((wq, wf, wi, wg)):
        part = jnp.dot(scaled, weight[...], preferred_element_type=f32)
        for head in range(heads):
            rows_scr[pl.ds(index * heads + head, rows, stride=step), :] = part[
                :, head * LANES : (head + 1) * LANES
            ]
    for row in range(4 * heads, step):
        rows_scr[pl.ds(row, rows, stride=step), :] = extra
    for row in range(rows):
        piece = rows_scr[pl.ds(row * step, step), :].reshape(out.shape[1:])
        out[OWNERS.index(row)] = piece.astype(bf16)


def recur_kernel(pieces, state, bound, gain, gated, forget_out, value_out, width):
    heads = state.shape[0]
    total = jnp.sum(pieces[...].astype(f32), axis=0)
    total = total.reshape(total.shape[0] * total.shape[1], LANES)
    squares = total[4 * heads : 4 * heads + 1, 0:1] + total[4 * heads : 4 * heads + 1, 1:2]
    row_scale = lax.rsqrt(squares / width + epsilon)
    query_pre, forget_pre, value_in, gate_pre = [
        row_scale * total[i * heads : (i + 1) * heads] for i in range(4)
    ]
    forget = bound[...] + (1.0 - bound[...]) * jax.nn.sigmoid(forget_pre)
    query_act = jax.nn.silu(query_pre)
    forget_out[...] = forget
    value_out[...] = value_in
    fresh = jnp.sum(query_act * (1.0 - forget), axis=1, keepdims=True) * value_in
    down = jnp.transpose(query_act * forget)
    reads = [
        jnp.sum(down[:, head : head + 1] * state[head], axis=0, keepdims=True)
        for head in range(heads)
    ]
    head_out = jnp.concatenate(reads, axis=0) + fresh
    head_out = head_out * lax.rsqrt(
        jnp.mean(head_out * head_out, axis=1, keepdims=True) + epsilon
    )
    value = (head_out * gain[...] * jax.nn.silu(gate_pre)).astype(bf16)
    for peer in range(gated.shape[0]):
        gated[peer] = value


def mix_kernel(own, other, tokens, weight, out, rows_scr, whole_scr):
    def body(team):
        rows = tokens.shape[0]
        heads = own.shape[1]
        for row in range(rows):
            place = slice(row * heads, (row + 1) * heads)
            side = 1 - team if TURNED[row] else team
            rows_scr[side, place, :] = own[ORDERS[team].index(row)].astype(f32)
            rows_scr[1 - side, place, :] = other[ORDERS[1 - team].index(row)].astype(f32)
        for side in range(2):
            for head in range(heads):
                column = (side * heads + head) * LANES
                whole_scr[:, column : column + LANES] = rows_scr[
                    side, pl.ds(head, rows, stride=heads), :
                ].astype(bf16)
        added = lax.dot_general(whole_scr[...], weight[...], NT, preferred_element_type=f32)
        mixed = tokens[...].astype(f32) + added
        half = rows // 2
        packed = jnp.concatenate([mixed[:half], mixed[half:]], axis=1)
        packed = (half_turn(packed) if team else packed).astype(bf16)
        for peer in range(out.shape[0]):
            out[peer] = packed

    for_my_team(body)


def part(index):
    return slice(index * LANES, (index + 1) * LANES)


def split_lanes(low, left, right):
    return jnp.where(low, left, half_turn(right)), jnp.where(low, half_turn(left), right)


def by_team(pair, halves):
    return halves[::-1] if TURNED[2 * pair] else halves


def arrange_in_kernel(w_gate, w_up, gain, forget, value, state, ins, gains, new_state):
    units = w_gate.shape[0]
    low = low_lanes((units, LANES))
    for pair in range(w_gate.shape[1] // (2 * LANES)):
        left, right = part(2 * pair), part(2 * pair + 1)
        for index, weight in enumerate((w_gate, w_up)):
            first, second = by_team(pair, split_lanes(low, weight[:, left], weight[:, right]))
            ins[0, index * units : (index + 1) * units, part(pair)] = first
            ins[1, index * units : (index + 1) * units, part(pair)] = second
        first, second = by_team(
            pair,
            split_lanes(
                low[:1], gain[2 * pair : 2 * pair + 1, :], gain[2 * pair + 1 : 2 * pair + 2, :]
            ),
        )
        gains[0, pair : pair + 1, :] = first
        gains[1, pair : pair + 1, :] = second
    down = jnp.transpose(forget[...])
    for head in range(state.shape[0]):
        keep = jnp.broadcast_to(down[:, head : head + 1], state.shape[1:])
        new_state[head] = keep * state[head] + (1.0 - keep) * value[head : head + 1, :]


def half_feed(team, chunk, gains, ins, scr):
    blocks, half, _ = chunk.shape
    low = low_lanes((half, LANES))
    squares = jnp.zeros((2 * half, LANES), f32)
    for pair in range(blocks // 2):
        first, second = split_lanes(
            low,
            chunk[ORDERS[team].index(2 * pair)].astype(f32),
            chunk[ORDERS[team].index(2 * pair + 1)].astype(f32),
        )
        value = jnp.concatenate([first, second], axis=0)
        squares = squares + value * value
        scr[:, part(pair)] = (value * gains[team, pair : pair + 1, :]).astype(bf16)
    products = lax.dot_general(scr[...], ins[team], NT, preferred_element_type=f32)
    return products, squares


def own_kernel(
    chunk, gains, ins, w_down, state, products, squares, outs, state_hbm, scr, sem
):
    store = pltpu.make_async_copy(state, state_hbm, sem)
    store.start()

    def body(team):
        products[...], squares[...] = half_feed(team, chunk, gains, ins, scr)

    for_my_team(body)
    low = low_lanes((w_down.shape[0], LANES))
    for pair in range(w_down.shape[1] // (2 * LANES)):
        first, second = by_team(
            pair, split_lanes(low, w_down[:, part(2 * pair)], w_down[:, part(2 * pair + 1)])
        )
        outs[0, :, part(pair)] = first
        outs[1, :, part(pair)] = second
    store.wait()


def packed_rows(low, block, turned):
    half = block.shape[0] // 2
    first, second = block[:half], block[half:]
    if turned:
        first, second = second, first
    return split_lanes(low, first, second)


def other_kernel(chunk, gains, ins, products, squares, outs, theirs, hidden_out, scr):
    def body(team):
        half = chunk.shape[1]
        more, more_squares = half_feed(1 - team, chunk, gains, ins, scr)
        totals = products[...] + jnp.concatenate([more[half:], more[:half]], axis=0)
        both = squares[...] + jnp.concatenate([more_squares[half:], more_squares[:half]], axis=0)
        mean = jnp.sum(both, axis=1, keepdims=True) / (chunk.shape[0] * LANES)
        totals = totals * lax.rsqrt(mean + epsilon)
        units = totals.shape[1] // 2
        hidden = (jax.nn.silu(totals[:, :units]) * totals[:, units:]).astype(bf16)
        hidden_out[...] = hidden
        terms = jnp.dot(hidden, outs[1 - team], preferred_element_type=f32)
        low = low_lanes((half, LANES))
        for pair in range(chunk.shape[0] // 2):
            left, right = packed_rows(low, terms[:, part(pair)], True)
            theirs[LAST_ORDERS[1 - team].index(2 * pair)] = left.astype(bf16)
            theirs[LAST_ORDERS[1 - team].index(2 * pair + 1)] = right.astype(bf16)

    for_my_team(body)


def mine_kernel(hidden, outs, mine):
    def body(team):
        terms = jnp.dot(hidden[...], outs[team], preferred_element_type=f32)
        low = low_lanes(mine.shape[1:])
        for pair in range(mine.shape[0] // 2):
            left, right = packed_rows(low, terms[:, part(pair)], False)
            mine[LAST_ORDERS[team].index(2 * pair)] = left
            mine[LAST_ORDERS[team].index(2 * pair + 1)] = right

    for_my_team(body)


def sum_kernel(mine, theirs, out):
    out[...] = (mine[...] + theirs[...].astype(f32)).astype(bf16)


def finish_kernel(pieces, mixed, out):
    half = mixed.shape[1]
    total = mixed[0].astype(f32) + jnp.sum(pieces[...].astype(f32), axis=0)
    total = jnp.where(my_team() == 0, total, half_turn(total))
    out[:half] = total[:, : LANES // 2].astype(bf16)
    out[half:] = half_turn(total)[:, : LANES // 2].astype(bf16)


def local(
    tokens,
    rec_state,
    norm_gain,
    w_query,
    w_forget,
    w_input,
    w_outgate,
    lower_bound,
    head_gain,
    w_heads_out,
    mixer_gain,
    w_gate,
    w_up,
    w_down,
):
    kv_count = lax.axis_size(KV)
    rows, cols = tokens.shape
    width = norm_gain.shape[0]
    heads = rec_state.shape[1]
    half = rows // 2
    blocks = width // LANES
    shape = pltpu.VMEM
    piece_rows = 4 * heads + 4

    other = lax.ppermute(tokens, "tp", SWAP)
    loads = (
        tokens,
        norm_gain.reshape(blocks, LANES),
        lower_bound.reshape(heads, LANES),
        head_gain.reshape(heads, LANES),
        mixer_gain.reshape(blocks, LANES),
    )
    tokens_here, first_gain, bound, gain, second_gain = pl.pallas_call(
        load_kernel,
        out_shape=tuple(shape(x.shape, x.dtype) for x in loads),
        in_specs=[IN_HBM] * len(loads),
        out_specs=tuple(in_vmem(len(loads))),
        scratch_shapes=[pltpu.SemaphoreType.DMA((len(loads),))],
        compiler_params=LIMIT,
        cost_estimate=pl.CostEstimate(flops=4000000000, bytes_accessed=20000000, transcendentals=0),
        name="load",
    )(*far(*loads))
    pieces = pl.pallas_call(
        project_kernel,
        out_shape=shape((rows, piece_rows // 4, 4, LANES), bf16),
        in_specs=in_vmem(7),
        out_specs=in_vmem(1)[0],
        scratch_shapes=[pltpu.VMEM((rows * piece_rows, LANES), f32)],
        compiler_params=LIMIT,
        name="project",
    )(
        *held(tokens_here, other, first_gain, w_query, w_forget, w_input, w_outgate)
    )
    pieces = exchanged(pieces, KV, [OWNERS])

    per_head = shape((heads, LANES), f32)
    gated, forget, value_in = pl.pallas_call(
        lambda *refs: recur_kernel(*refs, width),
        out_shape=(shape((kv_count, heads, LANES), bf16), per_head, per_head),
        in_specs=in_vmem(4),
        out_specs=tuple(in_vmem(3)),
        compiler_params=LIMIT,
        name="recur",
    )(*held(pieces, rec_state[0], bound, gain))

    own = exchanged(gated, KV_TP, teams(ORDERS))
    other = lax.ppermute(own, "tp", SWAP)
    mixed = pl.pallas_call(
        mix_kernel,
        out_shape=shape((kv_count, half, LANES), bf16),
        in_specs=in_vmem(4),
        out_specs=in_vmem(1)[0],
        scratch_shapes=[
            pltpu.VMEM((2, rows * heads, LANES), f32),
            pltpu.VMEM((rows, 2 * heads * LANES), bf16),
        ],
        compiler_params=LIMIT,
        name="mix",
    )(*held(own, other, tokens_here, w_heads_out.T))

    units = w_gate.shape[1]
    ins, gains, new_state = pl.pallas_call(
        arrange_in_kernel,
        out_shape=(
            shape((2, 2 * units, width // 2), bf16),
            shape((2, blocks // 2, LANES), f32),
            shape(rec_state.shape[1:], f32),
        ),
        in_specs=in_vmem(6),
        out_specs=tuple(in_vmem(3)),
        compiler_params=LIMIT,
        name="arrange_in",
    )(*held(w_gate.T, w_up.T, second_gain, forget, value_in, rec_state[0]))

    own = exchanged(mixed, KV_TP, teams(ORDERS))
    other = lax.ppermute(own, "tp", SWAP)
    chunks = (kv_count, half, LANES)
    products, squares, outs, new_state = pl.pallas_call(
        own_kernel,
        out_shape=(
            shape((rows, 2 * units), f32),
            shape((rows, LANES), f32),
            shape((2, units, width // 2), bf16),
            pltpu.HBM(new_state.shape, f32),
        ),
        in_specs=in_vmem(5),
        out_specs=tuple(in_vmem(3) + [IN_HBM]),
        scratch_shapes=[pltpu.VMEM((rows, width // 2), bf16), pltpu.SemaphoreType.DMA],
        compiler_params=LIMIT,
        name="own",
    )(*held(own, gains, ins, w_down, new_state))
    theirs, hidden = pl.pallas_call(
        other_kernel,
        out_shape=(shape(chunks, bf16), shape((rows, units), bf16)),
        in_specs=in_vmem(6),
        out_specs=tuple(in_vmem(2)),
        scratch_shapes=[pltpu.VMEM((rows, width // 2), bf16)],
        compiler_params=LIMIT,
        name="other",
    )(*held(other, gains, ins, products, squares, outs))
    mine = pl.pallas_call(
        mine_kernel,
        out_shape=shape(chunks, f32),
        in_specs=in_vmem(2),
        out_specs=in_vmem(1)[0],
        compiler_params=LIMIT,
        name="mine",
    )(*held(hidden, outs))
    theirs = lax.ppermute(theirs, "tp", SWAP)
    chip_sum = pl.pallas_call(
        sum_kernel,
        out_shape=shape((kv_count, half, LANES), bf16),
        in_specs=in_vmem(2),
        out_specs=in_vmem(1)[0],
        compiler_params=LIMIT,
        name="chip_sum",
    )(*held(mine, theirs))
    down = exchanged(chip_sum, KV_TP, teams(LAST_ORDERS))
    result = pl.pallas_call(
        finish_kernel,
        out_shape=jax.ShapeDtypeStruct((rows, cols), bf16),
        in_specs=in_vmem(2),
        out_specs=in_vmem(1)[0],
        compiler_params=LIMIT,
        name="finish",
    )(*held(down, mixed))
    return (result, new_state[None])


def solution(mesh):
    torus = Mesh(
        mesh.devices.reshape(mesh.shape["dp"], 8, 4, mesh.shape["tp"]), ("dp", "kv_0", "kv_1", "tp")
    )
    in_specs = (
        P("dp", KV_TP),
        P(DP_KV, "tp", None, None),
        P(),
        P(KV, "tp"),
        P(KV, "tp"),
        P(KV, "tp"),
        P(KV, "tp"),
        P("tp"),
        P("tp"),
        P(None, KV_TP),
        P(),
        P(None, KV_TP),
        P(None, KV_TP),
        P(KV_TP, None),
    )
    out_specs = (P("dp", KV_TP), P(DP_KV, "tp", None, None))


    return jax.shard_map(local, mesh=torus, in_specs=in_specs, out_specs=out_specs, check_vma=False)
```
